128 devices in a mesh: sp: 16 (over z, y), fs: 4 (over x), tp: 2 (over core).
Axes of the slice: x: 4, y: 4, z: 4, core: 2. Of those that a mesh axis runs over, the one named last changes fastest.
Arguments:
- tokens: bfloat16 [4, 32768, 2048], P('fs', 'sp'), may hold values from -21 to 21
- norm_gain: float32 [2048], replicated, may hold values from 0.1 to 1.9
- w_query: bfloat16 [2048, 1024], P(None, 'tp'), may hold values from -0.125 to 0.125
- w_key: bfloat16 [2048, 256], P(None, 'tp'), may hold values from -0.125 to 0.125
- w_value: bfloat16 [2048, 256], P(None, 'tp'), may hold values from -0.125 to 0.125
- w_pool: bfloat16 [2048, 1024], P(None, 'tp'), may hold values from -0.125 to 0.125
- w_group: bfloat16 [4, 256, 256], P('tp'), may hold values from -0.375 to 0.375
- w_out: bfloat16 [2048, 2048], replicated, may hold values from -0.125 to 0.125
- sinks: float32 [16], P('tp'), may hold values from -1 to 260
Outputs:
- mixed: bfloat16 [4, 32768, 2048], P('fs', ('sp', 'tp'))
- log_sums: float32 [4, 16, 32768], P('fs', 'tp', 'sp')
The draws below stay inside these ranges and needn't reach their ends.
All inputs are finite; a program needn't handle non-finite values.
Results may differ from the reference program's by a relative error of at most 0.009.
Values may be sent and summed in bfloat16 or wider, within the bound.
A program may use at most 192 MiB of HBM per device.

```python
import jax
import jax.numpy as jnp
from jax import lax

D = 2048
HEAD_SIZE = 64
QUERY_HEADS = 16
KEY_VALUE_HEADS = 4
GROUPS = 4
GDIM = 256
WINDOW_KEYS = 128
SEQS = 4
LEN = 32768
PW = 1024
QW = 1024
KW = 256


def draw_tokens(key, part):
    subkeys = jax.random.split(jax.random.fold_in(key, 11), 5)
    noise_part = jnp.clip(jax.random.normal(subkeys[0], (SEQS, LEN, D), jnp.float32), -4.0, 4.0)
    drift_sign = jnp.where(jax.random.uniform(subkeys[3], (SEQS, 1, 1), jnp.float32) < 0.5, -1.0, 1.0)
    drift_level = drift_sign * jax.random.uniform(subkeys[2], (SEQS, 1, 1), jnp.float32, 0.4, 1.0)
    rough_part = jax.random.uniform(subkeys[4], (SEQS, LEN // 32, 1), jnp.float32, -0.8, 0.8)
    direction = jnp.clip(jax.random.normal(subkeys[1], (SEQS, 1, D), jnp.float32), -3.0, 3.0)
    rise_factor = 1.0 + 2.0 * jnp.arange(LEN, dtype=jnp.float32)[None, :, None] / LEN
    amplitude = drift_level * rise_factor + jnp.repeat(rough_part, 32, axis=1)
    return (noise_part + amplitude * direction).astype(jnp.bfloat16)


def draw_sinks(key, part):
    subkeys = jax.random.split(jax.random.fold_in(key, 23), 1)
    sink_values = jax.random.uniform(subkeys[0], (QUERY_HEADS,), jnp.float32, -1.0, 6.0)
    return sink_values


def shard_levels(key, shape, pieces, smallest, high):
    factor_of, own = 1.0, jax.random.fold_in(key, 6)
    for position, shards_of in pieces:
        draws = jnp.exp(jax.random.uniform(jax.random.fold_in(own, position), (shards_of,), jnp.float32, smallest / len(pieces), high / len(pieces)))
        factor_of = factor_of * jnp.repeat(draws, shape[position] // shards_of).reshape([-1 if axis == position else 1 for axis in range(len(shape))])
    return factor_of


def scatter_about(stream_key, dims, width, bound, cuts=(), kind=jnp.bfloat16):
    entries = jax.random.normal(stream_key, dims, jnp.float32) * width
    if len(cuts) > 0:
        entries = shard_levels(stream_key, dims, cuts, -0.22, 0.18) * entries
    return jnp.clip(entries, min=-bound, max=bound).astype(kind)


def setup_inputs(seed: int = 0) -> dict:
    streams_of = jax.random.split(jax.random.key(seed), 10)
    return {
        "tokens": draw_tokens(jax.random.fold_in(streams_of[9], 71), 0),
        "norm_gain": jnp.clip(1.0 + 0.18 * jax.random.normal(streams_of[1], (D,), jnp.float32), 0.1, 1.9),
        "w_query": scatter_about(streams_of[2], (D, QW), D ** -0.5, 0.125, ((1, 2),)),
        "w_key": scatter_about(streams_of[3], (D, KW), D ** -0.5, 0.125, ((1, 2),)),
        "w_value": scatter_about(streams_of[4], (D, KW), D ** -0.5, 0.125, ((1, 2),)),
        "w_pool": scatter_about(streams_of[5], (D, PW), D ** -0.5, 0.125, ((1, 2),)),
        "w_group": scatter_about(streams_of[6], (GROUPS, GDIM, GDIM), GDIM ** -0.5, 0.375, ((0, 2),)),
        "w_out": scatter_about(streams_of[7], (PW + QW, D), (PW + QW) ** -0.5, 0.125),
        "sinks": draw_sinks(jax.random.fold_in(streams_of[9], 71), 0),
    }


LN_EPS = 1e-05

def normalize(token_rows, norm_gain):
    values = token_rows.astype(jnp.float32)
    row_mean = lax.optimization_barrier(jnp.mean(values, axis=-1, keepdims=True))
    centered = values - row_mean
    variance = lax.optimization_barrier(jnp.mean(centered * centered, axis=-1, keepdims=True))
    return (centered * lax.rsqrt(variance + LN_EPS) * norm_gain).astype(jnp.bfloat16)

def pool_branch(pool_rows, w_group):
    length = pool_rows.shape[0]
    reach = 2 ** GROUPS - 1
    values = pool_rows.astype(jnp.float32)
    padded = jnp.pad(values, ((reach, 0), (0, 0)))
    positions = jnp.arange(length, dtype=jnp.int32)
    prefix_mean = jnp.cumsum(values, axis=0) / (positions + 1).astype(jnp.float32)[:, None]
    outputs = []
    for group_index in range(GROUPS):
        span_width = 2 ** (group_index + 1)
        first_col = group_index * GDIM
        window_sum = jnp.zeros((length, GDIM), jnp.float32)
        for offset in range(span_width):
            window_sum = window_sum + padded[reach - offset:reach - offset + length, first_col:first_col + GDIM]
        window_count = jnp.minimum(positions + 1, span_width).astype(jnp.float32)[:, None]
        pooled = (window_sum / window_count - prefix_mean[:, first_col:first_col + GDIM]).astype(jnp.bfloat16)
        outputs.append(jnp.dot(pooled, w_group[group_index], preferred_element_type=jnp.float32).astype(jnp.bfloat16))
    return jnp.concatenate(outputs, axis=1)

def attention_branch(query_matrix, key_rows, value_rows, sinks):
    length = query_matrix.shape[0]
    block_extent = min(512, length)
    heads_per_group = QUERY_HEADS // KEY_VALUE_HEADS
    padded_keys = jnp.pad(key_rows, ((WINDOW_KEYS, 0), (0, 0)))
    padded_values = jnp.pad(value_rows, ((WINDOW_KEYS, 0), (0, 0)))
    attention_sink_logits = sinks.astype(jnp.float32).reshape(KEY_VALUE_HEADS, heads_per_group)[:, :, None, None]

    def one_block(block_index):
        start_row = (block_index * block_extent).astype(jnp.int32)
        query_tile_rows = lax.dynamic_slice_in_dim(query_matrix, start_row, block_extent, 0).reshape(block_extent, KEY_VALUE_HEADS, heads_per_group, HEAD_SIZE)
        key_tile_rows = lax.dynamic_slice_in_dim(padded_keys, start_row, block_extent + WINDOW_KEYS, 0).reshape(block_extent + WINDOW_KEYS, KEY_VALUE_HEADS, HEAD_SIZE)
        value_tile_rows = lax.dynamic_slice_in_dim(padded_values, start_row, block_extent + WINDOW_KEYS, 0).reshape(block_extent + WINDOW_KEYS, KEY_VALUE_HEADS, HEAD_SIZE)
        scores = jnp.einsum('qhrd,khd->hrqk', query_tile_rows.astype(jnp.float32), key_tile_rows.astype(jnp.float32)) * HEAD_SIZE ** (-0.5)
        query_positions = start_row + jnp.arange(block_extent, dtype=jnp.int32)
        key_positions = start_row - WINDOW_KEYS + jnp.arange(block_extent + WINDOW_KEYS, dtype=jnp.int32)
        distance = query_positions[:, None] - key_positions[None, :]
        visible = (distance >= 0) & (distance < WINDOW_KEYS) & (key_positions >= 0)[None, :]
        scores = jnp.where(visible, scores, -jnp.inf)
        row_max = jnp.maximum(lax.optimization_barrier(jnp.max(scores, axis=-1, keepdims=True)), attention_sink_logits)
        weights = jnp.exp(scores - row_max)
        weight_sum = lax.optimization_barrier(jnp.sum(weights, axis=-1, keepdims=True)) + jnp.exp(attention_sink_logits - row_max)
        normalized = (weights / weight_sum).astype(jnp.bfloat16)
        block_out = jnp.einsum('hrqk,khd->qhrd', normalized.astype(jnp.float32), value_tile_rows.astype(jnp.float32))
        block_out = block_out.astype(jnp.bfloat16).reshape(block_extent, QUERY_HEADS * HEAD_SIZE)
        block_logs = (row_max + jnp.log(weight_sum))[..., 0].reshape(QUERY_HEADS, block_extent)
        return (block_out, block_logs)
    block_outs, block_logs = lax.map(one_block, jnp.arange(length // block_extent, dtype=jnp.int32))
    attn_out = block_outs.reshape(length, QUERY_HEADS * HEAD_SIZE)
    log_sums = jnp.transpose(block_logs, (1, 0, 2)).reshape(QUERY_HEADS, length)
    return (attn_out, log_sums)

def reference(tokens, norm_gain, w_query, w_key, w_value, w_pool, w_group, w_out, sinks):

    def one_sequence(token_rows):
        normed = normalize(token_rows, norm_gain)
        query_matrix = jnp.dot(normed, w_query, preferred_element_type=jnp.float32).astype(jnp.bfloat16)
        key_rows = jnp.dot(normed, w_key, preferred_element_type=jnp.float32).astype(jnp.bfloat16)
        value_rows = jnp.dot(normed, w_value, preferred_element_type=jnp.float32).astype(jnp.bfloat16)
        pool_rows = jnp.dot(normed, w_pool, preferred_element_type=jnp.float32).astype(jnp.bfloat16)
        pool_out = pool_branch(pool_rows, w_group)
        attn_out, log_sums = attention_branch(query_matrix, key_rows, value_rows, sinks)
        joined = jnp.concatenate([pool_out, attn_out], axis=1)
        mixed = jnp.dot(joined, w_out, preferred_element_type=jnp.float32).astype(jnp.bfloat16)
        return (mixed, log_sums)
    mixed, log_sums = lax.map(one_sequence, tokens)
    return (mixed, log_sums)
```

```python
import functools

import jax
import jax.numpy as jnp
from jax import lax
from jax.experimental import pallas as pl
from jax.experimental.pallas import tpu as pltpu
from jax.sharding import PartitionSpec as P

HEAD_SIZE = 64
GROUPS = 4
GDIM = 256
WINDOW_KEYS = 128
QUERY_HEADS = 16
KEY_VALUE_HEADS = 4
LN_EPS = 1e-05

BLK = 128
HALO = 16
TILE = 256
F32, BF16 = jnp.float32, jnp.bfloat16


def mixer_kernel(
    sp_count,
    tok,
    gain,
    w_query,
    w_key,
    w_value,
    w_pool,
    w_group,
    sinks,
    acts_out,
    logs_out,
    X,
    W,
    WG,
    SK,
    PB,
    QT,
    KB,
    VT,
    ACT,
    LS,
    LSR,
    TOT,
    EARLIER,
    RECV,
    x_sem,
    w_sem,
    wsend_sem,
    wrecv_sem,
    hsend_sem,
    hrecv_sem,
    tsend_sem,
    trecv_sem,
    lsend_sem,
    lrecv_sem,
    act_sem,
    log_sem,
):
    rows = X.shape[0]
    blocks = rows // BLK
    width = X.shape[1]
    pw = PB.shape[1]
    qw = QT.shape[0]
    kw = KB.shape[1]
    half_p, half_q, half_k = pw // 2, qw // 2, kw // 2
    off_q, off_k, off_v = pw, pw + qw, pw + qw + kw
    sp, tp = lax.axis_index("sp"), lax.axis_index("tp")
    me = sp * 2 + tp
    count = sp_count * 2
    peer = {"tp": 1 - tp}
    heads = QUERY_HEADS
    own_heads = heads // 2

    def mesh_id(index):
        return {"sp": index // 2, "tp": lax.rem(index, 2)}

    def x_copy(b):
        return pltpu.make_async_copy(
            tok.at[pl.ds(pl.multiple_of(tp * rows + b * BLK, BLK), BLK), :],
            X.at[pl.ds(pl.multiple_of(b * BLK, BLK), BLK), :],
            x_sem.at[b],
        )

    @pl.loop(0, blocks)
    def _(b):
        x_copy(b).start()

    def cols(base, half):
        return pl.ds(pl.multiple_of(base + tp * half, 128), half)

    pieces = (
        (w_pool, W.at[:, cols(0, half_p)]),
        (w_query, W.at[:, cols(off_q, half_q)]),
        (w_key, W.at[:, cols(off_k, half_k)]),
        (w_value, W.at[:, cols(off_v, half_k)]),
        (w_group, WG.at[pl.ds(tp * 2, 2)]),
    )
    own_weights = [
        pltpu.make_async_copy(src, dst, w_sem.at[i]) for i, (src, dst) in enumerate(pieces)
    ]
    for copy in own_weights:
        copy.start()

    barrier = pltpu.get_barrier_semaphore()

    @pl.loop(1, count)
    def _(step):
        pl.semaphore_signal(
            barrier,
            inc=1,
            device_id=mesh_id(lax.rem(me + step, count)),
            device_id_type=pl.DeviceIdType.MESH,
        )

    own_sinks = pl.ds(pl.multiple_of(tp * own_heads, 8), own_heads)
    row_of = lax.broadcasted_iota(jnp.int32, (own_heads, 128), 0)
    sink_block = jnp.zeros((own_heads, 128), F32)
    for h in range(own_heads):
        sink_block = jnp.where(row_of == h, sinks[h], sink_block)
    SK[own_sinks, :] = sink_block

    first = me == 0

    @pl.when(first)
    def _():
        PB[0:HALO, :] = jnp.zeros((HALO, pw), BF16)
        KB[0:BLK, :] = jnp.zeros((BLK, kw), BF16)
        VT[:, 0:BLK] = jnp.zeros((kw, BLK), BF16)

    gains = gain[...]

    def norm_block(b):
        x_copy(b).wait()
        at = pl.ds(pl.multiple_of(b * BLK, BLK), BLK)
        values = X[at, :].astype(F32)
        mean = jnp.sum(values, axis=-1, keepdims=True) * (1.0 / width)
        centered = values - mean
        variance = jnp.sum(centered * centered, axis=-1, keepdims=True) * (1.0 / width)
        X[at, :] = (centered * lax.rsqrt(variance + LN_EPS) * gains).astype(BF16)

    early = 6

    @pl.loop(0, early)
    def _(b):
        norm_block(b)

    pl.semaphore_wait(barrier, count - 1)

    weight_sends = [
        pltpu.make_async_remote_copy(
            src_ref=src,
            dst_ref=dst,
            send_sem=wsend_sem.at[i],
            recv_sem=wrecv_sem.at[i],
            device_id=peer,
            device_id_type=pl.DeviceIdType.MESH,
        )
        for i, (src, dst) in enumerate(pieces + ((SK.at[own_sinks], SK.at[own_sinks]),))
    ]
    for i in (0, 2, 3, 1, 4, 5):
        weight_sends[i].start()

    @pl.loop(early, blocks)
    def _(b):
        norm_block(b)

    m_rows = 256

    def product(m, column):
        return jnp.dot(
            X[pl.ds(pl.multiple_of(m * m_rows, m_rows), m_rows), :],
            W[:, pl.ds(pl.multiple_of(column, TILE), TILE)],
            preferred_element_type=F32,
        )

    TOT[...] = jnp.zeros_like(TOT)

    def pool_tiles(which):
        @pl.loop(0, half_p // TILE)
        def _(j):
            column = pl.multiple_of(which * half_p + j * TILE, TILE)

            @pl.loop(0, rows // m_rows)
            def _(m):
                tile = product(m, column).astype(BF16)
                PB[pl.ds(pl.multiple_of(HALO + m * m_rows, HALO), m_rows), pl.ds(column, TILE)] = tile
                TOT[:, pl.ds(column, TILE)] += jnp.sum(tile.astype(F32), axis=0, keepdims=True)

    def query_tiles(which):
        @pl.loop(0, half_q // TILE)
        def _(j):
            column = pl.multiple_of(which * half_q + j * TILE, TILE)

            @pl.loop(0, rows // m_rows)
            def _(m):
                tile = (product(m, off_q + column) * (HEAD_SIZE**-0.5)).astype(BF16)
                QT[pl.ds(column, TILE), pl.ds(pl.multiple_of(m * m_rows, 128), m_rows)] = tile.T

    own_weights[0].wait()
    pool_tiles(tp)
    own_weights[1].wait()
    query_tiles(tp)
    weight_sends[0].wait_recv()
    pool_tiles(1 - tp)

    def total_copy(target, slot):
        return pltpu.make_async_remote_copy(
            src_ref=TOT,
            dst_ref=RECV.at[me],
            send_sem=tsend_sem.at[slot],
            recv_sem=trecv_sem.at[me],
            device_id=mesh_id(target),
            device_id_type=pl.DeviceIdType.MESH,
        )

    @pl.loop(1, count)
    def _(step):
        @pl.when(me + step < count)
        def _():
            total_copy(me + step, step).start()

    own_weights[2].wait()
    own_weights[3].wait()
    weight_sends[2].wait_recv()
    weight_sends[3].wait_recv()

    @pl.loop(0, rows // m_rows)
    def _(m):
        KB[pl.ds(pl.multiple_of(BLK + m * m_rows, BLK), m_rows), :] = product(m, off_k).astype(BF16)

    @pl.loop(0, rows // m_rows)
    def _(m):
        tile = product(m, off_v).astype(BF16)
        VT[:, pl.ds(pl.multiple_of(BLK + m * m_rows, BLK), m_rows)] = tile.T

    last = me == count - 1
    following = mesh_id(lax.rem(me + 1, count))
    halo_copies = [
        pltpu.make_async_remote_copy(
            src_ref=src,
            dst_ref=dst,
            send_sem=hsend_sem.at[i],
            recv_sem=hrecv_sem.at[i],
            device_id=following,
            device_id_type=pl.DeviceIdType.MESH,
        )
        for i, (src, dst) in enumerate(
            (
                (KB.at[pl.ds(rows, BLK)], KB.at[pl.ds(0, BLK)]),
                (VT.at[:, pl.ds(rows, BLK)], VT.at[:, pl.ds(0, BLK)]),
                (PB.at[pl.ds(rows, HALO)], PB.at[pl.ds(0, HALO)]),
            )
        )
    ]

    @pl.when(jnp.logical_not(last))
    def _():
        for copy in halo_copies:
            copy.start()

    weight_sends[1].wait_recv()
    query_tiles(1 - tp)
    weight_sends[4].wait_recv()
    weight_sends[5].wait_recv()
    own_weights[4].wait()

    lanes = (heads // KEY_VALUE_HEADS) * BLK
    per_kv = heads // KEY_VALUE_HEADS
    key_row = lax.broadcasted_iota(jnp.int32, (BLK, lanes), 0)
    query_lane = lax.broadcasted_iota(jnp.int32, (BLK, lanes), 1) & (BLK - 1)
    older = key_row > query_lane

    def act_copy(b, side):
        at = pl.ds(pl.multiple_of(b * BLK, BLK), BLK)
        side_cols = pl.ds(pl.multiple_of(side * pw, 128), pw)
        return pltpu.make_async_copy(
            ACT.at[at, side_cols], acts_out.at[at, side_cols], act_sem.at[side, b]
        )

    def attend(b, hide):
        start = pl.multiple_of(b * BLK, BLK)
        for g in range(KEY_VALUE_HEADS):
            key_part = KB[pl.ds(start, 2 * BLK), g * HEAD_SIZE : (g + 1) * HEAD_SIZE]
            query_part = jnp.concatenate(
                [
                    QT[(g * per_kv + r) * HEAD_SIZE : (g * per_kv + r + 1) * HEAD_SIZE, pl.ds(start, BLK)]
                    for r in range(per_kv)
                ],
                axis=1,
            )
            scores = jnp.dot(key_part, query_part, preferred_element_type=F32)
            before = scores[:BLK]
            if hide is not None:
                before = before + hide
            merged = jnp.where(older, before, scores[BLK:])
            sink = jnp.concatenate(
                [SK[g * per_kv + r : g * per_kv + r + 1, :] for r in range(per_kv)], axis=1
            )
            row_max = jnp.maximum(jnp.max(merged, axis=0, keepdims=True), sink)
            weights = jnp.exp(merged - row_max)
            weight_sum = jnp.sum(weights, axis=0, keepdims=True) + jnp.exp(sink - row_max)
            logs = row_max + jnp.log(weight_sum)
            for r in range(per_kv):
                LS[g * per_kv + r : g * per_kv + r + 1, pl.ds(start, BLK)] = logs[
                    :, r * BLK : (r + 1) * BLK
                ]
            spread = jnp.concatenate(
                [
                    jnp.where(older, weights, 0.0).astype(BF16),
                    jnp.where(older, 0.0, weights).astype(BF16),
                ],
                axis=0,
            )
            value_part = VT[g * HEAD_SIZE : (g + 1) * HEAD_SIZE, pl.ds(start, 2 * BLK)]
            mixed = jnp.dot(value_part, spread, preferred_element_type=F32)
            mixed = mixed * (1.0 / weight_sum)
            stacked = jnp.concatenate(
                [mixed[:, r * BLK : (r + 1) * BLK] for r in range(per_kv)], axis=0
            ).astype(BF16)
            ACT[pl.ds(start, BLK), pw + g * TILE : pw + (g + 1) * TILE] = stacked.T
        act_copy(b, 1).start()

    @pl.loop(1, blocks)
    def _(b):
        attend(b, None)

    @pl.when(jnp.logical_not(first))
    def _():
        for copy in halo_copies:
            copy.wait_recv()

    attend(0, jnp.where(first, -jnp.inf, 0.0).astype(F32))

    mine = pl.ds(pl.multiple_of(tp * rows, 128), rows)
    theirs = pl.ds(pl.multiple_of((1 - tp) * own_heads, 8), own_heads)
    log_swap = pltpu.make_async_remote_copy(
        src_ref=LS.at[theirs, :],
        dst_ref=LSR.at[:, mine],
        send_sem=lsend_sem,
        recv_sem=lrecv_sem,
        device_id=peer,
        device_id_type=pl.DeviceIdType.MESH,
    )
    log_swap.start()
    LSR[:, mine] = LS[own_sinks, :]

    EARLIER[...] = jnp.zeros_like(EARLIER)

    @pl.loop(0, count)
    def _(source):
        @pl.when(source < me)
        def _():
            pltpu.make_async_remote_copy(
                src_ref=TOT,
                dst_ref=RECV.at[source],
                send_sem=tsend_sem.at[0],
                recv_sem=trecv_sem.at[source],
                device_id=mesh_id(source),
                device_id_type=pl.DeviceIdType.MESH,
            ).wait_recv()
            EARLIER[...] += RECV[source]

    span = HALO + BLK
    out_row = lax.broadcasted_iota(jnp.int32, (BLK, span), 0)
    back = out_row + HALO - lax.broadcasted_iota(jnp.int32, (BLK, span), 1)
    in_block = lax.broadcasted_iota(jnp.int32, (BLK, span), 1) >= HALO
    prefix_ones = ((back >= 0) & in_block).astype(F32).astype(BF16)
    window_ones = [
        ((back >= 0) & (back < 2 ** (g + 1))).astype(F32).astype(BF16) for g in range(GROUPS)
    ]
    local_row = lax.broadcasted_iota(jnp.int32, (BLK, GDIM), 0)

    @pl.loop(0, blocks)
    def _(b):
        start = pl.multiple_of(b * BLK, BLK)
        seen = me * rows + b * BLK + 1 + local_row
        seen_float = seen.astype(F32)
        per_seen = 1.0 / seen_float
        for g in range(GROUPS):
            at_group = slice(g * GDIM, (g + 1) * GDIM)
            source = PB[pl.ds(pl.multiple_of(b * BLK, HALO), span), at_group]
            window_sum = jnp.dot(window_ones[g], source, preferred_element_type=F32)
            prefix = (
                jnp.dot(prefix_ones, source, preferred_element_type=F32) + EARLIER[:, at_group]
            )
            per_window = 1.0 / jnp.minimum(seen_float, float(2 ** (g + 1)))
            pooled = (window_sum * per_window - prefix * per_seen).astype(BF16)
            EARLIER[:, at_group] = prefix[BLK - 1 : BLK, :]
            ACT[pl.ds(start, BLK), at_group] = jnp.dot(
                pooled, WG[g], preferred_element_type=F32
            ).astype(BF16)
        act_copy(b, 0).start()

    log_swap.wait_recv()
    log_copy = pltpu.make_async_copy(LSR, logs_out, log_sem)
    log_copy.start()

    for copy in weight_sends:
        copy.wait_send()
    log_swap.wait_send()

    @pl.when(jnp.logical_not(last))
    def _():
        for copy in halo_copies:
            copy.wait_send()

    @pl.loop(1, count)
    def _(step):
        @pl.when(me + step < count)
        def _():
            total_copy(me + step, step).wait_send()

    @pl.loop(0, blocks)
    def _(b):
        act_copy(b, 0).wait()
        act_copy(b, 1).wait()

    log_copy.wait()


def output_kernel(acts, w_out, logs, mixed, logs_out):
    rows = acts.shape[0]
    m_rows = 256
    for m in range(rows // m_rows):
        at = slice(m * m_rows, (m + 1) * m_rows)
        mixed[at, :] = jnp.dot(acts[at, :], w_out[...], preferred_element_type=F32).astype(BF16)

    @pl.when(pl.program_id(0) == 0)
    def _():
        logs_out[...] = logs[...]


def body(sp_count, tokens, norm_gain, w_query, w_key, w_value, w_pool, w_group, w_out, sinks):
    token_rows = tokens[0]
    both_rows, width = token_rows.shape
    rows = both_rows // 2
    pw, qw, kw = 2 * w_pool.shape[1], 2 * w_query.shape[1], 2 * w_key.shape[1]
    count = sp_count * 2
    blocks = rows // BLK
    anywhere = pl.BlockSpec(memory_space=pl.ANY)
    dma = pltpu.SemaphoreType.DMA
    acts, logs = pl.pallas_call(
        functools.partial(mixer_kernel, sp_count),
        out_shape=(
            jax.ShapeDtypeStruct((rows, pw + qw), BF16),
            jax.ShapeDtypeStruct((QUERY_HEADS // 2, both_rows), F32),
        ),
        in_specs=[
            anywhere,
            pl.BlockSpec(memory_space=pltpu.VMEM),
            anywhere,
            anywhere,
            anywhere,
            anywhere,
            anywhere,
            pl.BlockSpec(memory_space=pltpu.SMEM),
        ],
        out_specs=(anywhere, anywhere),
        scratch_shapes=[
            pltpu.VMEM((rows, width), BF16),
            pltpu.VMEM((width, pw + qw + 2 * kw), BF16),
            pltpu.VMEM((GROUPS, GDIM, GDIM), BF16),
            pltpu.VMEM((QUERY_HEADS, 128), F32),
            pltpu.VMEM((HALO + rows, pw), BF16),
            pltpu.VMEM((qw, rows), BF16),
            pltpu.VMEM((BLK + rows, kw), BF16),
            pltpu.VMEM((kw, BLK + rows), BF16),
            pltpu.VMEM((rows, pw + qw), BF16),
            pltpu.VMEM((QUERY_HEADS, rows), F32),
            pltpu.VMEM((QUERY_HEADS // 2, both_rows), F32),
            pltpu.VMEM((1, pw), F32),
            pltpu.VMEM((1, pw), F32),
            pltpu.VMEM((count, 1, pw), F32),
            dma((blocks,)),
            dma((5,)),
            dma((6,)),
            dma((6,)),
            dma((3,)),
            dma((3,)),
            dma((count,)),
            dma((count,)),
            dma,
            dma,
            dma((2, blocks)),
            dma,
        ],
        compiler_params=pltpu.CompilerParams(
            collective_id=0, has_side_effects=True, vmem_limit_bytes=44 * 2**20
        ),
        name="mixers",
    )(token_rows, norm_gain[None, :], w_query, w_key, w_value, w_pool, w_group, sinks)

    out_tile = 256
    mixed, log_sums = pl.pallas_call(
        output_kernel,
        grid=(w_out.shape[1] // out_tile,),
        out_shape=(
            jax.ShapeDtypeStruct((rows, w_out.shape[1]), BF16),
            jax.ShapeDtypeStruct((QUERY_HEADS // 2, both_rows), F32),
        ),
        in_specs=[
            pl.BlockSpec((rows, pw + qw), lambda n: (0, 0)),
            pl.BlockSpec((pw + qw, out_tile), lambda n: (0, n)),
            pl.BlockSpec((QUERY_HEADS // 2, both_rows), lambda n: (0, 0)),
        ],
        out_specs=(
            pl.BlockSpec((rows, out_tile), lambda n: (0, n)),
            pl.BlockSpec((QUERY_HEADS // 2, both_rows), lambda n: (0, 0)),
        ),
        compiler_params=pltpu.CompilerParams(
            dimension_semantics=("arbitrary",), vmem_limit_bytes=30 * 2**20
        ),
        name="output",
    )(acts, w_out, logs)
    return mixed[None], log_sums[None]


def solution(mesh):
    return jax.shard_map(
        functools.partial(body, mesh.shape["sp"]),
        mesh=mesh,
        in_specs=(
            P("fs", "sp", None),
            P(),
            P(None, "tp"),
            P(None, "tp"),
            P(None, "tp"),
            P(None, "tp"),
            P("tp", None, None),
            P(),
            P("tp"),
        ),
        out_specs=(P("fs", ("sp", "tp"), None), P("fs", "tp", "sp")),
        check_vma=False,
    )
```

```python
import functools

import jax
import jax.numpy as jnp
from jax import lax
from jax.experimental import pallas as pl
from jax.experimental.pallas import tpu as pltpu
from jax.sharding import PartitionSpec as P

HEAD_SIZE = 64
GROUPS = 4
GDIM = 256
WINDOW_KEYS = 128
QUERY_HEADS = 16
KEY_VALUE_HEADS = 4
LN_EPS = 1e-05

BLK = 128
HALO = 16
TILE = 256
F32, BF16 = jnp.float32, jnp.bfloat16


MESH = pl.DeviceIdType.MESH
PART = 4


def project_kernel(
    tok,
    gain,
    w_query,
    w_key,
    w_value,
    w_pool,
    w_group,
    sinks,
    X,
    WP,
    WQ,
    WKV,
    WG,
    SK,
    PA,
    QA,
    TA,
    GAIN,
    SINK,
    WPO,
    WQO,
    x_sem,
    w_sem,
    small_sem,
    send_sem,
    recv_sem,
):
    rows, width = X.shape
    blocks = rows // BLK
    half_k = WKV.shape[1] // 4
    own_heads = QUERY_HEADS // 2
    tp = lax.axis_index("tp")
    peer = {"tp": 1 - tp}

    barrier = pltpu.get_barrier_semaphore()
    pl.semaphore_signal(barrier, inc=1, device_id=peer, device_id_type=MESH)

    small = [
        pltpu.make_async_copy(gain, GAIN, small_sem.at[0]),
        pltpu.make_async_copy(sinks, SINK, small_sem.at[1]),
    ]
    for copy in small:
        copy.start()

    def x_copy(b):
        return pltpu.make_async_copy(
            tok.at[pl.ds(pl.multiple_of(tp * rows + b * BLK, BLK), BLK), :],
            X.at[pl.ds(pl.multiple_of(b * BLK, BLK), BLK), :],
            x_sem.at[b],
        )

    @pl.loop(0, blocks)
    def _(b):
        x_copy(b).start()

    own = [
        pltpu.make_async_copy(src, dst, w_sem.at[i])
        for i, (src, dst) in enumerate(
            (
                (w_pool, WPO),
                (w_query, WQO),
                (w_key, WKV.at[:, 0:half_k]),
                (w_value, WKV.at[:, 2 * half_k : 3 * half_k]),
                (w_group, WG.at[0 : GROUPS // 2]),
            )
        )
    ]
    for copy in own:
        copy.start()

    for copy in small:
        copy.wait()
    row_of = lax.broadcasted_iota(jnp.int32, (own_heads, 128), 0)
    sink_block = jnp.zeros((own_heads, 128), F32)
    for h in range(own_heads):
        sink_block = jnp.where(row_of == h, SINK[h], sink_block)
    SK[0:own_heads, :] = sink_block

    pl.semaphore_wait(barrier, 1)
    sends = [
        pltpu.make_async_remote_copy(
            src_ref=src,
            dst_ref=dst,
            send_sem=send_sem.at[i],
            recv_sem=recv_sem.at[i],
            device_id=peer,
            device_id_type=MESH,
        )
        for i, (src, dst) in enumerate(
            (
                (w_pool, WP),
                (w_key, WKV.at[:, half_k : 2 * half_k]),
                (w_value, WKV.at[:, 3 * half_k : 4 * half_k]),
                (w_query, WQ),
                (w_group, WG.at[GROUPS // 2 : GROUPS]),
                (SK.at[0:own_heads], SK.at[own_heads : 2 * own_heads]),
            )
        )
    ]
    for copy in sends:
        copy.start()

    gains = GAIN[...]

    @pl.loop(0, blocks)
    def _(b):
        x_copy(b).wait()
        at = pl.ds(pl.multiple_of(b * BLK, BLK), BLK)
        values = X[at, :].astype(F32)
        mean = jnp.sum(values, axis=-1, keepdims=True) * (1.0 / width)
        centered = values - mean
        variance = jnp.sum(centered * centered, axis=-1, keepdims=True) * (1.0 / width)
        X[at, :] = (centered * lax.rsqrt(variance + LN_EPS) * gains).astype(BF16)

    own[0].wait()
    tile = jnp.dot(X[...], WPO[...], preferred_element_type=F32).astype(BF16)
    PA[...] = tile
    TA[...] = jnp.sum(tile.astype(F32), axis=0, keepdims=True)
    own[1].wait()
    tile = jnp.dot(X[...], WQO[...], preferred_element_type=F32) * (HEAD_SIZE**-0.5)
    QA[...] = tile.astype(BF16).T

    for copy in own[2:]:
        copy.wait()
    for copy in sends:
        copy.wait()


def mixer_kernel(
    sp_count,
    X,
    WP,
    WQ,
    WKV,
    WG,
    SK,
    PA,
    QA,
    TA,
    ACT,
    LSR,
    PB,
    QB,
    KB,
    VT,
    PH,
    KH,
    VH,
    LS,
    TOT,
    EARLIER,
    RECV,
    BAND,
    hsend_sem,
    hrecv_sem,
    tsend_sem,
    trecv_sem,
    lsend_sem,
    lrecv_sem,
):
    rows, kw = KB.shape
    half_p, half_q, half_k = PA.shape[1], QA.shape[0], kw // 2
    pw, qw = 2 * half_p, 2 * half_q
    blocks = rows // BLK
    sp, tp = lax.axis_index("sp"), lax.axis_index("tp")
    me = sp * 2 + tp
    count = sp_count * 2
    own_heads = QUERY_HEADS // 2
    first, last = me == 0, me == count - 1

    def mesh_id(index):
        return {"sp": index // 2, "tp": lax.rem(index, 2)}

    barrier = pltpu.get_barrier_semaphore()

    @pl.loop(1, count)
    def _(step):
        pl.semaphore_signal(
            barrier,
            inc=1,
            device_id=mesh_id(lax.rem(me + step, count)),
            device_id_type=MESH,
        )

    @pl.when(first)
    def _():
        PH[...] = jnp.zeros_like(PH)
        KH[...] = jnp.zeros_like(KH)
        VH[...] = jnp.zeros_like(VH)

    tile = jnp.dot(X[...], WP[...], preferred_element_type=F32).astype(BF16)
    PB[...] = tile
    TOT[pl.ds(tp, 1), 0] = TA[...]
    TOT[pl.ds(1 - tp, 1), 0] = jnp.sum(tile.astype(F32), axis=0, keepdims=True)
    tile = jnp.dot(X[...], WKV[...], preferred_element_type=F32).astype(BF16)
    KB[...] = tile[:, :kw]
    VT[...] = tile[:, kw:].T
    tile = jnp.dot(X[...], WQ[...], preferred_element_type=F32) * (HEAD_SIZE**-0.5)
    QB[...] = tile.astype(BF16).T

    tail, own_k, other_k = slice(rows - BLK, rows), slice(0, half_k), slice(half_k, kw)
    halo_copies = [
        pltpu.make_async_remote_copy(
            src_ref=src,
            dst_ref=dst,
            send_sem=hsend_sem.at[i],
            recv_sem=hrecv_sem.at[i],
            device_id=mesh_id(lax.rem(me + 1, count)),
            device_id_type=MESH,
        )
        for i, (src, dst) in enumerate(
            (
                (KB.at[tail, own_k], KH.at[:, other_k]),
                (KB.at[tail, other_k], KH.at[:, own_k]),
                (VT.at[own_k, tail], VH.at[other_k, :]),
                (VT.at[other_k, tail], VH.at[own_k, :]),
                (PA.at[rows - HALO : rows], PH.at[1]),
                (PB.at[rows - HALO : rows], PH.at[0]),
            )
        )
    ]

    def total_copy(target, slot):
        return pltpu.make_async_remote_copy(
            src_ref=TOT,
            dst_ref=RECV.at[me],
            send_sem=tsend_sem.at[slot],
            recv_sem=trecv_sem.at[me],
            device_id=mesh_id(target),
            device_id_type=MESH,
        )

    pl.semaphore_wait(barrier, count - 1)

    @pl.when(jnp.logical_not(last))
    def _():
        for copy in halo_copies:
            copy.start()

    @pl.loop(1, count)
    def _(step):
        @pl.when(me + step < count)
        def _():
            total_copy(me + step, step).start()

    span = HALO + BLK
    pairs = 2 * BLK
    older = lax.broadcasted_iota(jnp.int32, (BLK, pairs), 0) > (
        lax.broadcasted_iota(jnp.int32, (BLK, pairs), 1) & (BLK - 1)
    )
    back = (
        lax.broadcasted_iota(jnp.int32, (BLK, span), 0)
        + HALO
        - lax.broadcasted_iota(jnp.int32, (BLK, span), 1)
    )
    in_block = lax.broadcasted_iota(jnp.int32, (BLK, span), 1) >= HALO
    prefix_ones = jnp.where((back >= 0) & in_block, 1.0, 0.0).astype(BF16)
    groups = [lax.rem(2 * tp + j, GROUPS) for j in range(GROUPS)]
    reaches = [jnp.left_shift(jnp.int32(2), group) for group in groups]
    for j, reach in enumerate(reaches):
        BAND[j, 0:BLK, :] = jnp.where(
            (back >= 0) & (back < reach), 1.0 / reach.astype(F32), 0.0
        ).astype(BF16)
        BAND[j, BLK : 2 * BLK, :] = prefix_ones

    per_kv = QUERY_HEADS // KEY_VALUE_HEADS

    def attend(b, hide):
        start = pl.multiple_of(b * BLK, BLK)
        ahead = pl.ds(start, BLK)
        both = pl.ds(pl.multiple_of(start - BLK, BLK), 2 * BLK)

        def query_rows(h):
            source, row = (QA, h) if h < own_heads else (QB, h - own_heads)
            return source[row * HEAD_SIZE : (row + 1) * HEAD_SIZE, ahead]

        def attend_part(first_group, last_group):
            units = []
            for g in range(first_group, last_group):
                at_head = slice(g * HEAD_SIZE, (g + 1) * HEAD_SIZE)
                if hide is None:
                    key_part = KB[both, at_head]
                    value_part = VT[at_head, both]
                else:
                    key_part = jnp.concatenate([KH[:, at_head], KB[0:BLK, at_head]], axis=0)
                    value_part = jnp.concatenate([VH[at_head, :], VT[at_head, 0:BLK]], axis=1)
                for h in range(g * per_kv, (g + 1) * per_kv, 2):
                    query_part = jnp.concatenate(
                        [query_rows(h), query_rows(h + 1)], axis=1
                    )
                    sink = jnp.concatenate([SK[h : h + 1, :], SK[h + 1 : h + 2, :]], axis=1)
                    score = jnp.dot(key_part, query_part, preferred_element_type=F32)
                    units.append((h, score, value_part, sink))
            results = []
            for h, score, value_part, sink in units:
                before = score[:BLK]
                if hide is not None:
                    before = before + hide
                merged = jnp.where(older, before, score[BLK:])
                row_max = jnp.maximum(jnp.max(merged, axis=0, keepdims=True), sink)
                weights = jnp.exp(merged - row_max)
                weight_sum = jnp.sum(weights, axis=0, keepdims=True) + jnp.exp(sink - row_max)
                spread = jnp.concatenate(
                    [
                        jnp.where(older, weights, 0.0).astype(BF16),
                        jnp.where(older, 0.0, weights).astype(BF16),
                    ],
                    axis=0,
                )
                mixed = jnp.dot(value_part, spread, preferred_element_type=F32)
                mixed = mixed * (1.0 / weight_sum)
                stacked = jnp.concatenate([mixed[:, :BLK], mixed[:, BLK:]], axis=0).astype(BF16)
                results.append((h, stacked.T, row_max + jnp.log(weight_sum)))
            for h, out, logs in results:
                LS[h : h + 1, ahead] = logs[:, :BLK]
                LS[h + 1 : h + 2, ahead] = logs[:, BLK:]
                column = pw + lax.rem(tp * half_q + h * HEAD_SIZE, qw)
                ACT[ahead, pl.ds(pl.multiple_of(column, 128), 2 * HEAD_SIZE)] = out

        for g in range(0, KEY_VALUE_HEADS, PART):
            attend_part(g, g + PART)

    @pl.loop(1, blocks)
    def _(b):
        attend(b, None)

    @pl.when(jnp.logical_not(first))
    def _():
        for copy in halo_copies:
            copy.wait_recv()

    attend(0, jnp.where(first, -jnp.inf, 0.0).astype(F32))

    mine = pl.ds(pl.multiple_of(tp * rows, 128), rows)
    log_swap = pltpu.make_async_remote_copy(
        src_ref=LS.at[own_heads : 2 * own_heads, :],
        dst_ref=LSR.at[:, mine],
        send_sem=lsend_sem,
        recv_sem=lrecv_sem,
        device_id={"tp": 1 - tp},
        device_id_type=MESH,
    )
    log_swap.start()
    LSR[:, mine] = LS[0:own_heads, :]

    EARLIER[...] = jnp.zeros_like(EARLIER)

    @pl.loop(0, count)
    def _(source):
        @pl.when(source < me)
        def _():
            pltpu.make_async_remote_copy(
                src_ref=TOT,
                dst_ref=RECV.at[source],
                send_sem=tsend_sem.at[0],
                recv_sem=trecv_sem.at[source],
                device_id=mesh_id(source),
                device_id_type=MESH,
            ).wait_recv()
            EARLIER[...] += RECV[source]

    local_row = lax.broadcasted_iota(jnp.int32, (BLK, 128), 0)

    def pool(b, opening):
        start = pl.multiple_of(b * BLK, BLK)
        seen = (me * rows + b * BLK + 1 + local_row).astype(F32)
        per_seen = 1.0 / seen
        per_seen = jnp.concatenate([per_seen, per_seen], axis=1)
        sums, befores, carries, outs = [], [], [], []
        for j in range(GROUPS):
            side, at_group = j // 2, slice((j % 2) * GDIM, (j % 2 + 1) * GDIM)
            held = PA if side == 0 else PB
            if opening:
                source = jnp.concatenate([PH[side, :, at_group], held[0:BLK, at_group]], axis=0)
            else:
                source = held[pl.ds(pl.multiple_of(start - HALO, HALO), span), at_group]
            sums.append(jnp.dot(BAND[j], source, preferred_element_type=F32))
            befores.append(EARLIER[pl.ds(tp if side == 0 else 1 - tp, 1), 0, at_group])
        for j in range(GROUPS):
            window_mean = sums[j][:BLK]
            if opening:
                reach = reaches[j].astype(F32)
                fewer = reach / jnp.minimum(seen, reach)
                window_mean = window_mean * jnp.concatenate([fewer, fewer], axis=1)
            prefix = sums[j][BLK:] + befores[j]
            carries.append(prefix[BLK - 1 : BLK, :])
            pooled = (window_mean - prefix * per_seen).astype(BF16)
            outs.append(jnp.dot(pooled, WG[j], preferred_element_type=F32).astype(BF16))
        for j in range(GROUPS):
            side, at_group = j // 2, slice((j % 2) * GDIM, (j % 2 + 1) * GDIM)
            EARLIER[pl.ds(tp if side == 0 else 1 - tp, 1), 0, at_group] = carries[j]
            column = pl.multiple_of(groups[j] * GDIM, GDIM)
            ACT[pl.ds(start, BLK), pl.ds(column, GDIM)] = outs[j]

    pool(0, True)

    @pl.loop(1, blocks)
    def _(b):
        pool(b, False)

    log_swap.wait()

    @pl.when(jnp.logical_not(last))
    def _():
        for copy in halo_copies:
            copy.wait_send()

    @pl.loop(1, count)
    def _(step):
        @pl.when(me + step < count)
        def _():
            total_copy(me + step, step).wait_send()


def output_kernel(acts, w_out, logs, mixed_out, logs_out, MIXED, out_sem, log_sem):
    rows, width = MIXED.shape
    n_cols = 512
    log_copy = pltpu.make_async_copy(logs, logs_out, log_sem)
    log_copy.start()

    def out_copy(n):
        at = pl.ds(pl.multiple_of(n * n_cols, n_cols), n_cols)
        return pltpu.make_async_copy(MIXED.at[:, at], mixed_out.at[:, at], out_sem.at[n])

    @pl.loop(0, width // n_cols)
    def _(n):
        column = pl.ds(pl.multiple_of(n * n_cols, n_cols), n_cols)
        MIXED[:, column] = jnp.dot(
            acts[...], w_out[:, column], preferred_element_type=F32
        ).astype(BF16)
        out_copy(n).start()

    @pl.loop(0, width // n_cols)
    def _(n):
        out_copy(n).wait()

    log_copy.wait()


def body(sp_count, tokens, norm_gain, w_query, w_key, w_value, w_pool, w_group, w_out, sinks):
    token_rows = tokens[0]
    both_rows, width = token_rows.shape
    rows = both_rows // 2
    pw, qw, kw = 2 * w_pool.shape[1], 2 * w_query.shape[1], 2 * w_key.shape[1]
    count = sp_count * 2
    blocks = rows // BLK
    hbm = pl.BlockSpec(memory_space=pltpu.HBM)
    vmem = pl.BlockSpec(memory_space=pltpu.VMEM)
    dma = pltpu.SemaphoreType.DMA
    arguments = (
        token_rows,
        norm_gain[None, :],
        w_query,
        w_key,
        w_value,
        w_pool,
        w_group,
        sinks,
    )
    projected = pl.pallas_call(
        project_kernel,
        out_shape=(
            jax.ShapeDtypeStruct((rows, width), BF16),
            jax.ShapeDtypeStruct((width, pw // 2), BF16),
            jax.ShapeDtypeStruct((width, qw // 2), BF16),
            jax.ShapeDtypeStruct((width, 2 * kw), BF16),
            jax.ShapeDtypeStruct((GROUPS, GDIM, GDIM), BF16),
            jax.ShapeDtypeStruct((QUERY_HEADS, 128), F32),
            jax.ShapeDtypeStruct((rows, pw // 2), BF16),
            jax.ShapeDtypeStruct((qw // 2, rows), BF16),
            jax.ShapeDtypeStruct((1, pw // 2), F32),
        ),
        in_specs=[hbm] * 8,
        out_specs=(vmem,) * 9,
        scratch_shapes=[
            pltpu.VMEM((1, width), F32),
            pltpu.SMEM((QUERY_HEADS // 2,), F32),
            pltpu.VMEM((width, pw // 2), BF16),
            pltpu.VMEM((width, qw // 2), BF16),
            dma((blocks,)),
            dma((5,)),
            dma((2,)),
            dma((6,)),
            dma((6,)),
        ],
        compiler_params=pltpu.CompilerParams(
            collective_id=0, has_side_effects=True, vmem_limit_bytes=24 * 2**20
        ),
        name="project",
    )(*(pltpu.with_memory_space_constraint(array, pltpu.HBM) for array in arguments))

    acts, logs = pl.pallas_call(
        functools.partial(mixer_kernel, sp_count),
        out_shape=(
            jax.ShapeDtypeStruct((rows, pw + qw), BF16),
            jax.ShapeDtypeStruct((QUERY_HEADS // 2, both_rows), F32),
        ),
        in_specs=[vmem] * 9,
        out_specs=(vmem, vmem),
        scratch_shapes=[
            pltpu.VMEM((rows, pw // 2), BF16),
            pltpu.VMEM((qw // 2, rows), BF16),
            pltpu.VMEM((rows, kw), BF16),
            pltpu.VMEM((kw, rows), BF16),
            pltpu.VMEM((2, HALO, pw // 2), BF16),
            pltpu.VMEM((BLK, kw), BF16),
            pltpu.VMEM((kw, BLK), BF16),
            pltpu.VMEM((QUERY_HEADS, rows), F32),
            pltpu.VMEM((2, 1, pw // 2), F32),
            pltpu.VMEM((2, 1, pw // 2), F32),
            pltpu.VMEM((count, 2, 1, pw // 2), F32),
            pltpu.VMEM((GROUPS, 2 * BLK, HALO + BLK), BF16),
            dma((6,)),
            dma((6,)),
            dma((count,)),
            dma((count,)),
            dma,
            dma,
        ],
        compiler_params=pltpu.CompilerParams(
            collective_id=1, has_side_effects=True, vmem_limit_bytes=28 * 2**20
        ),
        name="mixers",
    )(*projected)

    n_cols = 512
    mixed, log_sums = pl.pallas_call(
        output_kernel,
        out_shape=(
            jax.ShapeDtypeStruct((rows, w_out.shape[1]), BF16),
            jax.ShapeDtypeStruct((QUERY_HEADS // 2, both_rows), F32),
        ),
        in_specs=[vmem, vmem, vmem],
        out_specs=(hbm, hbm),
        scratch_shapes=[
            pltpu.VMEM((rows, w_out.shape[1]), BF16),
            dma((w_out.shape[1] // n_cols,)),
            dma,
        ],
        compiler_params=pltpu.CompilerParams(vmem_limit_bytes=20 * 2**20),
        name="output",
    )(acts, w_out, logs)
    return mixed[None], log_sums[None]


def solution(mesh):
    return jax.shard_map(
        functools.partial(body, mesh.shape["sp"]),
        mesh=mesh,
        in_specs=(
            P("fs", "sp", None),
            P(),
            P(None, "tp"),
            P(None, "tp"),
            P(None, "tp"),
            P(None, "tp"),
            P("tp", None, None),
            P(),
            P("tp"),
        ),
        out_specs=(P("fs", ("sp", "tp"), None), P("fs", "tp", "sp")),
        check_vma=False,
    )
```

```python
import functools

import jax
import jax.numpy as jnp
from jax import lax
from jax.experimental import pallas as pl
from jax.experimental.pallas import tpu as pltpu
from jax.sharding import PartitionSpec as P

HEAD_SIZE = 64
GROUPS = 4
GDIM = 256
WINDOW_KEYS = 128
QUERY_HEADS = 16
KEY_VALUE_HEADS = 4
LN_EPS = 1e-05

BLK = 128
HALO = 16
TILE = 256
F32, BF16 = jnp.float32, jnp.bfloat16


MESH = pl.DeviceIdType.MESH
NORM_ROWS = 128
NORM_TILE = 256
STEPS = (512,)
AHEAD = 6


def project_kernel(
    tok,
    gain,
    w_query,
    w_key,
    w_value,
    w_pool,
    w_group,
    sinks,
    X,
    WP,
    WQ,
    WKV,
    WG,
    SK,
    PA,
    QA,
    KA,
    VA,
    TA,
    GAIN,
    GAINS,
    SINK,
    WPO,
    WQO,
    WKVO,
    x_sem,
    w_sem,
    small_sem,
    send_sem,
    recv_sem,
):
    rows, width = X.shape
    blocks = rows // BLK
    half_p, half_q, half_k = PA.shape[1], QA.shape[0], KA.shape[1]
    own_heads = QUERY_HEADS // 2
    tp = lax.axis_index("tp")
    peer = {"tp": 1 - tp}

    barrier = pltpu.get_barrier_semaphore()
    pl.semaphore_signal(barrier, inc=1, device_id=peer, device_id_type=MESH)

    small = [
        pltpu.make_async_copy(gain, GAIN, small_sem.at[0]),
        pltpu.make_async_copy(sinks, SINK, small_sem.at[1]),
    ]
    for copy in small:
        copy.start()

    def x_copy(b):
        return pltpu.make_async_copy(
            tok.at[pl.ds(pl.multiple_of(tp * rows + b * BLK, BLK), BLK), :],
            X.at[b * BLK : (b + 1) * BLK, :],
            x_sem.at[b],
        )

    for b in range(blocks):
        x_copy(b).start()

    pl.semaphore_wait(barrier, 1)
    sends = [
        pltpu.make_async_remote_copy(
            src_ref=src,
            dst_ref=dst,
            send_sem=send_sem.at[i],
            recv_sem=recv_sem.at[i],
            device_id=peer,
            device_id_type=MESH,
        )
        for i, (src, dst) in enumerate(
            (
                (w_pool, WP),
                (w_key, WKV.at[:, 0:half_k]),
                (w_value, WKV.at[:, half_k : 2 * half_k]),
                (w_query, WQ),
                (w_group, WG.at[GROUPS // 2 : GROUPS]),
                (SK.at[0:own_heads], SK.at[own_heads : 2 * own_heads]),
            )
        )
    ]
    for copy in sends[:5]:
        copy.start()

    own = [
        pltpu.make_async_copy(src, dst, w_sem.at[i])
        for i, (src, dst) in enumerate(
            (
                (w_pool, WPO),
                (w_query, WQO),
                (w_key, WKVO.at[:, 0:half_k]),
                (w_value, WKVO.at[:, half_k : 2 * half_k]),
                (w_group, WG.at[0 : GROUPS // 2]),
            )
        )
    ]
    for copy in own:
        copy.start()

    for copy in small:
        copy.wait()
    row_of = lax.broadcasted_iota(jnp.int32, (own_heads, 128), 0)
    sink_block = jnp.zeros((own_heads, 128), F32)
    for h in range(own_heads):
        sink_block = jnp.where(row_of == h, SINK[h], sink_block)
    SK[0:own_heads, :] = sink_block

    GAINS[...] = jnp.broadcast_to(GAIN[...], GAINS.shape)

    def normalized(row):
        values = X[row : row + NORM_ROWS, :].astype(F32)
        mean = jnp.sum(values, axis=-1, keepdims=True) * (1.0 / width)
        centered = values - mean
        variance = jnp.sum(centered * centered, axis=-1, keepdims=True) * (1.0 / width)
        scaled = (centered * lax.rsqrt(variance + LN_EPS)).reshape(-1, 8, width)
        return (scaled * GAINS[...][None]).reshape(NORM_ROWS, width).astype(BF16)

    def project(first_row, last_row, normed_to):
        at = slice(first_row, last_row)
        todo = list(range(last_row, normed_to, NORM_ROWS))
        slots = (half_p + half_q) // NORM_TILE
        following, pools, queries = [], [], []
        rows_in = X[at, :]

        def norm_some(slot):
            for row in todo[len(todo) * slot // slots : len(todo) * (slot + 1) // slots]:
                following.append((row, normalized(row)))

        for n in range(0, half_p, NORM_TILE):
            pools.append(jnp.dot(rows_in, WPO[:, n : n + NORM_TILE], preferred_element_type=F32))
            norm_some(n // NORM_TILE)
        for n in range(0, half_q, NORM_TILE):
            queries.append(jnp.dot(rows_in, WQO[:, n : n + NORM_TILE], preferred_element_type=F32))
            norm_some((half_p + n) // NORM_TILE)
        both = jnp.dot(rows_in, WKVO[...], preferred_element_type=F32).astype(BF16)
        for row, block in following:
            X[row : row + NORM_ROWS, :] = block
        for index, pool in enumerate(pools):
            columns = slice(index * NORM_TILE, (index + 1) * NORM_TILE)
            rounded = pool.astype(BF16)
            PA[at, columns] = rounded
            total = jnp.sum(rounded.astype(F32), axis=0, keepdims=True)
            TA[:, columns] = total if first_row == 0 else TA[:, columns] + total
        for index, query in enumerate(queries):
            at_rows = slice(index * NORM_TILE, (index + 1) * NORM_TILE)
            QA[at_rows, at] = (query * (HEAD_SIZE**-0.5)).astype(BF16).T
        KA[at, :] = both[:, :half_k]
        VA[:, at] = both[:, half_k:].T

    for row in range(0, STEPS[0], NORM_ROWS):
        x_copy(row // BLK).wait()
        X[row : row + NORM_ROWS, :] = normalized(row)
    for b in range(STEPS[0] // BLK, blocks):
        x_copy(b).wait()
    sends[5].start()
    for copy in own:
        copy.wait()
    bounds = (0, *STEPS, rows, rows)
    for step in range(len(bounds) - 2):
        project(*bounds[step : step + 3])

    for copy in sends:
        copy.wait()


def mixer_kernel(
    sp_count,
    X,
    WP,
    WQ,
    WKV,
    WG,
    SK,
    PA,
    QA,
    KA,
    VA,
    TA,
    w_out,
    ACT,
    LSR,
    WO,
    PB,
    QB,
    KB,
    VB,
    PH,
    KH,
    VH,
    LS,
    TOT,
    EARLIER,
    RECV,
    KEEP,
    BAND,
    hsend_sem,
    hrecv_sem,
    tsend_sem,
    trecv_sem,
    lsend_sem,
    lrecv_sem,
    out_sem,
):
    rows, half_k = KB.shape
    half_p, half_q = PA.shape[1], QA.shape[0]
    pw, qw = 2 * half_p, 2 * half_q
    blocks = rows // BLK
    sp, tp = lax.axis_index("sp"), lax.axis_index("tp")
    me = sp * 2 + tp
    count = sp_count * 2
    own_heads = QUERY_HEADS // 2
    first, last = me == 0, me == count - 1

    out_copy = pltpu.make_async_copy(w_out, WO, out_sem)
    out_copy.start()

    barrier = pltpu.get_barrier_semaphore()

    def arrive(device):
        pl.semaphore_signal(barrier, inc=1, device_id=device, device_id_type=MESH)

    arrive({"tp": 1 - tp})
    for distance in range(1, sp_count):
        place = sp + distance
        place = jnp.where(place >= sp_count, place - sp_count, place)
        for core in range(2):
            arrive({"sp": place, "tp": core})

    @pl.when(first)
    def _():
        PH[...] = jnp.zeros_like(PH)
        KH[...] = jnp.zeros_like(KH)
        VH[...] = jnp.zeros_like(VH)

    tile = jnp.dot(X[...], WP[...], preferred_element_type=F32).astype(BF16)
    PB[...] = tile
    TOT[pl.ds(tp, 1), 0] = TA[...]
    TOT[pl.ds(1 - tp, 1), 0] = jnp.sum(tile.astype(F32), axis=0, keepdims=True)
    tile = jnp.dot(X[...], WKV[...], preferred_element_type=F32).astype(BF16)
    KB[...] = tile[:, :half_k]
    VB[...] = tile[:, half_k:].T
    tile = jnp.dot(X[...], WQ[...], preferred_element_type=F32) * (HEAD_SIZE**-0.5)
    QB[...] = tile.astype(BF16).T

    tail = slice(rows - BLK, rows)
    following = lax.rem(sp + tp, sp_count)
    halo_copies = [
        pltpu.make_async_remote_copy(
            src_ref=src,
            dst_ref=dst,
            send_sem=hsend_sem.at[i],
            recv_sem=hrecv_sem.at[i],
            device_id={"sp": following, "tp": 1 - tp},
            device_id_type=MESH,
        )
        for i, (src, dst) in enumerate(
            (
                (KA.at[tail, :], KH.at[1]),
                (KB.at[tail, :], KH.at[0]),
                (VA.at[:, tail], VH.at[1]),
                (VB.at[:, tail], VH.at[0]),
                (PA.at[rows - HALO : rows], PH.at[1]),
                (PB.at[rows - HALO : rows], PH.at[0]),
            )
        )
    ]

    def total_copy(place, core, source):
        return pltpu.make_async_remote_copy(
            src_ref=TOT,
            dst_ref=RECV.at[source],
            send_sem=tsend_sem.at[place * 2 + core],
            recv_sem=trecv_sem.at[source],
            device_id={"sp": place, "tp": core},
            device_id_type=MESH,
        )

    def for_later(act):
        @pl.when(tp == 0)
        def _():
            act(sp, 1)

        @pl.loop(sp + 1, sp_count)
        def _(place):
            act(place, 0)
            act(place, 1)

    pl.semaphore_wait(barrier, count - 1)

    @pl.when(jnp.logical_not(last))
    def _():
        for copy in halo_copies:
            copy.start()

    for_later(lambda place, core: total_copy(place, core, me).start())

    span = HALO + BLK
    pairs = 2 * BLK
    older = lax.broadcasted_iota(jnp.int32, (BLK, pairs), 0) > (
        lax.broadcasted_iota(jnp.int32, (BLK, pairs), 1) & (BLK - 1)
    )
    KEEP[0] = jnp.where(older, 1.0, 0.0).astype(BF16)
    KEEP[1] = jnp.where(older, 0.0, 1.0).astype(BF16)
    back = (
        lax.broadcasted_iota(jnp.int32, (BLK, span), 0)
        + HALO
        - lax.broadcasted_iota(jnp.int32, (BLK, span), 1)
    )
    in_block = lax.broadcasted_iota(jnp.int32, (BLK, span), 1) >= HALO
    prefix_ones = jnp.where((back >= 0) & in_block, 1.0, 0.0).astype(BF16)
    groups = [lax.rem(2 * tp + j, GROUPS) for j in range(GROUPS)]
    reaches = [jnp.left_shift(jnp.int32(2), group) for group in groups]
    for j, reach in enumerate(reaches):
        BAND[j, 0:BLK, :] = jnp.where(
            (back >= 0) & (back < reach), 1.0 / reach.astype(F32), 0.0
        ).astype(BF16)
        BAND[j, BLK : 2 * BLK, :] = prefix_ones

    per_kv = QUERY_HEADS // KEY_VALUE_HEADS

    def query_rows(h, ahead):
        source, row = (QA, h) if h < own_heads else (QB, h - own_heads)
        return source[row * HEAD_SIZE : (row + 1) * HEAD_SIZE, ahead]

    kv_side = KEY_VALUE_HEADS // 2

    def attend(*spec):
        units = []
        for b, hide in spec:
            start = pl.multiple_of(b * BLK, BLK)
            for h in range(0, QUERY_HEADS, 2):
                units.append((start, hide, h))
        parts = {}

        def ask(index):
            start, hide, h = units[index]
            ahead = pl.ds(start, BLK)
            both = pl.ds(pl.multiple_of(start - BLK, BLK), 2 * BLK)
            side, slot = divmod(h // per_kv, kv_side)
            keys, values = (KA, VA) if side == 0 else (KB, VB)
            at_head = slice(slot * HEAD_SIZE, (slot + 1) * HEAD_SIZE)
            if hide is None:
                key_part, value_part = keys[both, at_head], values[at_head, both]
            else:
                key_part = jnp.concatenate([KH[side, :, at_head], keys[0:BLK, at_head]], axis=0)
                value_part = jnp.concatenate([VH[side, at_head, :], values[at_head, 0:BLK]], axis=1)
            query_part = jnp.concatenate([query_rows(h, ahead), query_rows(h + 1, ahead)], axis=1)
            sink = jnp.concatenate([SK[h : h + 1, :], SK[h + 1 : h + 2, :]], axis=1)
            score = jnp.dot(key_part, query_part, preferred_element_type=F32)
            parts[index] = (ahead, hide, h, score, value_part, sink)

        for index in range(min(AHEAD, len(units))):
            ask(index)
        results = []
        for index in range(len(units)):
            ahead, hide, h, score, value_part, sink = parts.pop(index)
            before = score[:BLK]
            if hide is not None:
                before = before + hide
            merged = jnp.where(older, before, score[BLK:])
            row_max = jnp.maximum(jnp.max(merged, axis=0, keepdims=True), sink)
            weights = jnp.exp(merged - row_max)
            weight_sum = jnp.sum(weights, axis=0, keepdims=True) + jnp.exp(sink - row_max)
            rounded = weights.astype(BF16)
            if index + AHEAD < len(units):
                ask(index + AHEAD)
            spread = jnp.concatenate([rounded * KEEP[0], rounded * KEEP[1]], axis=0)
            mixed = jnp.dot(value_part, spread, preferred_element_type=F32)
            mixed = mixed * (1.0 / weight_sum)
            stacked = jnp.concatenate([mixed[:, :BLK], mixed[:, BLK:]], axis=0).astype(BF16)
            results.append((ahead, h, stacked.T, row_max + jnp.log(weight_sum)))
        for ahead, h, out, logs in results:
            LS[h : h + 1, ahead] = logs[:, :BLK]
            LS[h + 1 : h + 2, ahead] = logs[:, BLK:]
            column = pw + lax.rem(tp * half_q + h * HEAD_SIZE, qw)
            ACT[ahead, pl.ds(pl.multiple_of(column, 128), 2 * HEAD_SIZE)] = out

    @pl.loop(1, blocks // 2)
    def _(b):
        attend((2 * b, None), (2 * b + 1, None))

    @pl.when(jnp.logical_not(first))
    def _():
        for copy in halo_copies:
            copy.wait_recv()

    attend((1, None), (0, jnp.where(first, -jnp.inf, 0.0).astype(F32)))

    mine = pl.ds(pl.multiple_of(tp * rows, 128), rows)
    log_swap = pltpu.make_async_remote_copy(
        src_ref=LS.at[own_heads : 2 * own_heads, :],
        dst_ref=LSR.at[:, mine],
        send_sem=lsend_sem,
        recv_sem=lrecv_sem,
        device_id={"tp": 1 - tp},
        device_id_type=MESH,
    )
    log_swap.start()
    LSR[:, mine] = LS[0:own_heads, :]

    @pl.loop(0, sp)
    def _(place):
        total_copy(place, 0, place * 2).wait_recv()
        total_copy(place, 1, place * 2 + 1).wait_recv()

    @pl.when(tp == 1)
    def _():
        total_copy(sp, 0, sp * 2).wait_recv()

    earlier = jnp.zeros(EARLIER.shape, F32)
    for source in range(count - 1):
        earlier += jnp.where(source < me, RECV[source], 0.0)
    EARLIER[...] = earlier

    local_row = lax.broadcasted_iota(jnp.int32, (BLK, 128), 0)

    def pool(*spec):
        units = []
        for b, opening in spec:
            start = pl.multiple_of(b * BLK, BLK)
            for j in range(GROUPS):
                side, at_group = j // 2, slice((j % 2) * GDIM, (j % 2 + 1) * GDIM)
                held = PA if side == 0 else PB
                if opening:
                    source = jnp.concatenate([PH[side, :, at_group], held[0:BLK, at_group]], axis=0)
                else:
                    source = held[pl.ds(pl.multiple_of(start - HALO, HALO), span), at_group]
                units.append(jnp.dot(BAND[j], source, preferred_element_type=F32))
        sides = [pl.ds(tp if j < 2 else 1 - tp, 1) for j in range(GROUPS)]
        carries = [
            EARLIER[sides[j], 0, (j % 2) * GDIM : (j % 2 + 1) * GDIM] for j in range(GROUPS)
        ]
        outs = []
        for (b, opening), sums in zip(spec, zip(*[iter(units)] * GROUPS)):
            seen = (me * rows + b * BLK + 1 + local_row).astype(F32)
            per_seen = 1.0 / seen
            per_seen = jnp.concatenate([per_seen, per_seen], axis=1)
            for j in range(GROUPS):
                window_mean = sums[j][:BLK]
                if opening:
                    reach = reaches[j].astype(F32)
                    fewer = reach / jnp.minimum(seen, reach)
                    window_mean = window_mean * jnp.concatenate([fewer, fewer], axis=1)
                prefix = sums[j][BLK:] + carries[j]
                carries[j] = prefix[BLK - 1 : BLK, :]
                pooled = (window_mean - prefix * per_seen).astype(BF16)
                out = jnp.dot(pooled, WG[j], preferred_element_type=F32).astype(BF16)
                outs.append((pl.ds(pl.multiple_of(b * BLK, BLK), BLK), groups[j], out))
        for j in range(GROUPS):
            EARLIER[sides[j], 0, (j % 2) * GDIM : (j % 2 + 1) * GDIM] = carries[j]
        for at, group, out in outs:
            ACT[at, pl.ds(pl.multiple_of(group * GDIM, GDIM), GDIM)] = out

    pool((0, True), (1, False))

    @pl.loop(1, blocks // 2)
    def _(b):
        pool((2 * b, False), (2 * b + 1, False))

    out_copy.wait()
    log_swap.wait()

    @pl.when(jnp.logical_not(last))
    def _():
        for copy in halo_copies:
            copy.wait_send()

    for_later(lambda place, core: total_copy(place, core, me).wait_send())


def output_kernel(acts, w_out, logs, mixed_out, logs_out, MIXED, out_sem, log_sem):
    rows, width = MIXED.shape
    n_cols = 512
    log_copy = pltpu.make_async_copy(logs, logs_out, log_sem)
    log_copy.start()

    def out_copy(n):
        at = pl.ds(pl.multiple_of(n * n_cols, n_cols), n_cols)
        return pltpu.make_async_copy(MIXED.at[:, at], mixed_out.at[:, at], out_sem.at[n])

    @pl.loop(0, width // n_cols)
    def _(n):
        column = pl.ds(pl.multiple_of(n * n_cols, n_cols), n_cols)
        MIXED[:, column] = jnp.dot(
            acts[...], w_out[:, column], preferred_element_type=F32
        ).astype(BF16)
        out_copy(n).start()

    @pl.loop(0, width // n_cols)
    def _(n):
        out_copy(n).wait()

    log_copy.wait()


def body(sp_count, tokens, norm_gain, w_query, w_key, w_value, w_pool, w_group, w_out, sinks):
    token_rows = tokens[0]
    both_rows, width = token_rows.shape
    rows = both_rows // 2
    pw, qw, kw = 2 * w_pool.shape[1], 2 * w_query.shape[1], 2 * w_key.shape[1]
    count = sp_count * 2
    blocks = rows // BLK
    hbm = pl.BlockSpec(memory_space=pltpu.HBM)
    vmem = pl.BlockSpec(memory_space=pltpu.VMEM)
    dma = pltpu.SemaphoreType.DMA
    arguments = (
        token_rows,
        norm_gain[None, :],
        w_query,
        w_key,
        w_value,
        w_pool,
        w_group,
        sinks,
    )
    projected = pl.pallas_call(
        project_kernel,
        out_shape=(
            jax.ShapeDtypeStruct((rows, width), BF16),
            jax.ShapeDtypeStruct((width, pw // 2), BF16),
            jax.ShapeDtypeStruct((width, qw // 2), BF16),
            jax.ShapeDtypeStruct((width, kw), BF16),
            jax.ShapeDtypeStruct((GROUPS, GDIM, GDIM), BF16),
            jax.ShapeDtypeStruct((QUERY_HEADS, 128), F32),
            jax.ShapeDtypeStruct((rows, pw // 2), BF16),
            jax.ShapeDtypeStruct((qw // 2, rows), BF16),
            jax.ShapeDtypeStruct((rows, kw // 2), BF16),
            jax.ShapeDtypeStruct((kw // 2, rows), BF16),
            jax.ShapeDtypeStruct((1, pw // 2), F32),
        ),
        in_specs=[hbm] * 8,
        out_specs=(vmem,) * 11,
        scratch_shapes=[
            pltpu.VMEM((1, width), F32),
            pltpu.VMEM((8, width), F32),
            pltpu.SMEM((QUERY_HEADS // 2,), F32),
            pltpu.VMEM((width, pw // 2), BF16),
            pltpu.VMEM((width, qw // 2), BF16),
            pltpu.VMEM((width, kw), BF16),
            dma((blocks,)),
            dma((5,)),
            dma((2,)),
            dma((6,)),
            dma((6,)),
        ],
        compiler_params=pltpu.CompilerParams(
            collective_id=0, has_side_effects=True, vmem_limit_bytes=20 * 2**20
        ),
        name="project",
    )(*(pltpu.with_memory_space_constraint(array, pltpu.HBM) for array in arguments))

    acts, logs, out_weights = pl.pallas_call(
        functools.partial(mixer_kernel, sp_count),
        out_shape=(
            jax.ShapeDtypeStruct((rows, pw + qw), BF16),
            jax.ShapeDtypeStruct((QUERY_HEADS // 2, both_rows), F32),
            jax.ShapeDtypeStruct(w_out.shape, BF16),
        ),
        in_specs=[vmem] * 11 + [hbm],
        out_specs=(vmem, vmem, vmem),
        scratch_shapes=[
            pltpu.VMEM((rows, pw // 2), BF16),
            pltpu.VMEM((qw // 2, rows), BF16),
            pltpu.VMEM((rows, kw // 2), BF16),
            pltpu.VMEM((kw // 2, rows), BF16),
            pltpu.VMEM((2, HALO, pw // 2), BF16),
            pltpu.VMEM((2, BLK, kw // 2), BF16),
            pltpu.VMEM((2, kw // 2, BLK), BF16),
            pltpu.VMEM((QUERY_HEADS, rows), F32),
            pltpu.VMEM((2, 1, pw // 2), F32),
            pltpu.VMEM((2, 1, pw // 2), F32),
            pltpu.VMEM((count, 2, 1, pw // 2), F32),
            pltpu.VMEM((2, BLK, 2 * BLK), BF16),
            pltpu.VMEM((GROUPS, 2 * BLK, HALO + BLK), BF16),
            dma((6,)),
            dma((6,)),
            dma((count,)),
            dma((count,)),
            dma,
            dma,
            dma,
        ],
        compiler_params=pltpu.CompilerParams(
            collective_id=1, has_side_effects=True, vmem_limit_bytes=20 * 2**20
        ),
        name="mixers",
    )(*projected, pltpu.with_memory_space_constraint(w_out, pltpu.HBM))

    n_cols = 512
    mixed, log_sums = pl.pallas_call(
        output_kernel,
        out_shape=(
            jax.ShapeDtypeStruct((rows, w_out.shape[1]), BF16),
            jax.ShapeDtypeStruct((QUERY_HEADS // 2, both_rows), F32),
        ),
        in_specs=[vmem, vmem, vmem],
        out_specs=(hbm, hbm),
        scratch_shapes=[
            pltpu.VMEM((rows, w_out.shape[1]), BF16),
            dma((w_out.shape[1] // n_cols,)),
            dma,
        ],
        compiler_params=pltpu.CompilerParams(vmem_limit_bytes=20 * 2**20),
        name="output",
    )(acts, out_weights, logs)
    return mixed[None], log_sums[None]


def solution(mesh):
    return jax.shard_map(
        functools.partial(body, mesh.shape["sp"]),
        mesh=mesh,
        in_specs=(
            P("fs", "sp", None),
            P(),
            P(None, "tp"),
            P(None, "tp"),
            P(None, "tp"),
            P(None, "tp"),
            P("tp", None, None),
            P(),
            P("tp"),
        ),
        out_specs=(P("fs", ("sp", "tp"), None), P("fs", "tp", "sp")),
        check_vma=False,
    )
```

```python
import functools

import jax
import jax.numpy as jnp
from jax import lax
from jax.experimental import pallas as pl
from jax.experimental.pallas import tpu as pltpu
from jax.sharding import PartitionSpec as P

HEAD_SIZE = 64
GROUPS = 4
GDIM = 256
WINDOW_KEYS = 128
QUERY_HEADS = 16
KEY_VALUE_HEADS = 4
LN_EPS = 1e-05

BLK = 128
HALO = 16
TILE = 256
F32, BF16 = jnp.float32, jnp.bfloat16


MESH = pl.DeviceIdType.MESH
NORM_ROWS = 128
NORM_TILE = 256
OUT_TILE = 512
SEND_STEP = 2
WG_INDEX, PA_INDEX = 4, 6
STEPS = (512,)
AHEAD = 6


def project_kernel(
    tok,
    gain,
    w_query,
    w_key,
    w_value,
    w_pool,
    w_group,
    sinks,
    X,
    WP,
    WQ,
    WKV,
    WG,
    SK,
    PA,
    QA,
    KA,
    VA,
    TA,
    GAIN,
    GAINS,
    SINK,
    WPO,
    WQO,
    WKVO,
    x_sem,
    w_sem,
    small_sem,
    send_sem,
    recv_sem,
):
    rows, width = X.shape
    blocks = rows // BLK
    half_p, half_q, half_k = PA.shape[1], QA.shape[0], KA.shape[1]
    own_heads = QUERY_HEADS // 2
    tp = lax.axis_index("tp")
    peer = {"tp": 1 - tp}

    barrier = pltpu.get_barrier_semaphore()
    pl.semaphore_signal(barrier, inc=1, device_id=peer, device_id_type=MESH)

    small = [
        pltpu.make_async_copy(gain, GAIN, small_sem.at[0]),
        pltpu.make_async_copy(sinks, SINK, small_sem.at[1]),
    ]
    for copy in small:
        copy.start()

    def x_copy(b):
        return pltpu.make_async_copy(
            tok.at[pl.ds(pl.multiple_of(tp * rows + b * BLK, BLK), BLK), :],
            X.at[b * BLK : (b + 1) * BLK, :],
            x_sem.at[b],
        )

    for b in range(blocks):
        x_copy(b).start()

    pl.semaphore_wait(barrier, 1)
    sends = [
        pltpu.make_async_remote_copy(
            src_ref=src,
            dst_ref=dst,
            send_sem=send_sem.at[i],
            recv_sem=recv_sem.at[i],
            device_id=peer,
            device_id_type=MESH,
        )
        for i, (src, dst) in enumerate(
            (
                (w_pool, WP),
                (w_key, WKV.at[:, 0:half_k]),
                (w_value, WKV.at[:, half_k : 2 * half_k]),
                (w_query, WQ),
                (w_group, WG.at[GROUPS // 2 : GROUPS]),
                (SK.at[0:own_heads], SK.at[own_heads : 2 * own_heads]),
            )
        )
    ]
    for copy in sends[:5]:
        copy.start()

    own = [
        pltpu.make_async_copy(src, dst, w_sem.at[i])
        for i, (src, dst) in enumerate(
            (
                (w_pool, WPO),
                (w_query, WQO),
                (w_key, WKVO.at[:, 0:half_k]),
                (w_value, WKVO.at[:, half_k : 2 * half_k]),
                (w_group, WG.at[0 : GROUPS // 2]),
            )
        )
    ]
    for copy in own:
        copy.start()

    for copy in small:
        copy.wait()
    row_of = lax.broadcasted_iota(jnp.int32, (own_heads, 128), 0)
    sink_block = jnp.zeros((own_heads, 128), F32)
    for h in range(own_heads):
        sink_block = jnp.where(row_of == h, SINK[h], sink_block)
    SK[0:own_heads, :] = sink_block

    GAINS[...] = jnp.broadcast_to(GAIN[...], GAINS.shape)

    def normalized(row):
        values = X[row : row + NORM_ROWS, :].astype(F32)
        mean = jnp.sum(values, axis=-1, keepdims=True) * (1.0 / width)
        centered = values - mean
        variance = jnp.sum(centered * centered, axis=-1, keepdims=True) * (1.0 / width)
        scaled = (centered * lax.rsqrt(variance + LN_EPS)).reshape(-1, 8, width)
        return (scaled * GAINS[...][None]).reshape(NORM_ROWS, width).astype(BF16)

    def project(first_row, last_row, normed_to):
        at = slice(first_row, last_row)
        todo = list(range(last_row, normed_to, NORM_ROWS))
        slots = (half_p + half_q) // NORM_TILE
        following, pools, queries = [], [], []
        rows_in = X[at, :]

        def norm_some(slot):
            for row in todo[len(todo) * slot // slots : len(todo) * (slot + 1) // slots]:
                following.append((row, normalized(row)))

        for n in range(0, half_p, NORM_TILE):
            pools.append(jnp.dot(rows_in, WPO[:, n : n + NORM_TILE], preferred_element_type=F32))
            norm_some(n // NORM_TILE)
        for n in range(0, half_q, NORM_TILE):
            queries.append(jnp.dot(rows_in, WQO[:, n : n + NORM_TILE], preferred_element_type=F32))
            norm_some((half_p + n) // NORM_TILE)
        both = jnp.dot(rows_in, WKVO[...], preferred_element_type=F32).astype(BF16)
        for row, block in following:
            X[row : row + NORM_ROWS, :] = block
        for index, pool in enumerate(pools):
            columns = slice(index * NORM_TILE, (index + 1) * NORM_TILE)
            rounded = pool.astype(BF16)
            PA[at, columns] = rounded
            total = jnp.sum(rounded.astype(F32), axis=0, keepdims=True)
            TA[:, columns] = total if first_row == 0 else TA[:, columns] + total
        for index, query in enumerate(queries):
            at_rows = slice(index * NORM_TILE, (index + 1) * NORM_TILE)
            QA[at_rows, at] = (query * (HEAD_SIZE**-0.5)).astype(BF16).T
        KA[at, :] = both[:, :half_k]
        VA[:, at] = both[:, half_k:].T

    for row in range(0, STEPS[0], NORM_ROWS):
        x_copy(row // BLK).wait()
        X[row : row + NORM_ROWS, :] = normalized(row)
    for b in range(STEPS[0] // BLK, blocks):
        x_copy(b).wait()
    sends[5].start()
    for copy in own:
        copy.wait()
    bounds = (0, *STEPS, rows, rows)
    for step in range(len(bounds) - 2):
        project(*bounds[step : step + 3])

    for copy in sends:
        copy.wait()


def mixer_kernel(
    sp_count,
    X,
    WP,
    WQ,
    WKV,
    WG,
    SK,
    PA,
    QA,
    KA,
    VA,
    TA,
    w_out,
    PART,
    LSR,
    PB,
    PH,
    EARLIER,
    WOP,
    ATT,
    WOA,
    QB,
    KB,
    VB,
    KH,
    VH,
    LS,
    TOT,
    RECV,
    KEEP,
    hsend_sem,
    hrecv_sem,
    tsend_sem,
    trecv_sem,
    lsend_sem,
    lrecv_sem,
    out_sem,
):
    rows, half_k = KB.shape
    half_p, half_q = PA.shape[1], QA.shape[0]
    pw, qw = 2 * half_p, 2 * half_q
    blocks = rows // BLK
    sp, tp = lax.axis_index("sp"), lax.axis_index("tp")
    me = sp * 2 + tp
    count = sp_count * 2
    own_heads = QUERY_HEADS // 2
    first, last = me == 0, me == count - 1

    out_copies = [
        pltpu.make_async_copy(w_out.at[pw : pw + qw], WOA, out_sem.at[0]),
        pltpu.make_async_copy(w_out.at[0:pw], WOP, out_sem.at[1]),
    ]
    for copy in out_copies:
        copy.start()

    barrier = pltpu.get_barrier_semaphore()

    def arrive(device):
        pl.semaphore_signal(barrier, inc=1, device_id=device, device_id_type=MESH)

    arrive({"tp": 1 - tp})
    for distance in range(1, sp_count):
        place = sp + distance
        place = jnp.where(place >= sp_count, place - sp_count, place)
        for core in range(2):
            arrive({"sp": place, "tp": core})

    @pl.when(first)
    def _():
        PH[...] = jnp.zeros_like(PH)
        KH[...] = jnp.zeros_like(KH)
        VH[...] = jnp.zeros_like(VH)

    tile = jnp.dot(X[...], WP[...], preferred_element_type=F32).astype(BF16)
    PB[...] = tile
    TOT[pl.ds(tp, 1), 0] = TA[...]
    TOT[pl.ds(1 - tp, 1), 0] = jnp.sum(tile.astype(F32), axis=0, keepdims=True)
    tile = jnp.dot(X[...], WKV[...], preferred_element_type=F32).astype(BF16)
    KB[...] = tile[:, :half_k]
    VB[...] = tile[:, half_k:].T
    tile = jnp.dot(X[...], WQ[...], preferred_element_type=F32) * (HEAD_SIZE**-0.5)
    QB[...] = tile.astype(BF16).T

    tail = slice(rows - BLK, rows)
    following = lax.rem(sp + tp, sp_count)
    halo_copies = [
        pltpu.make_async_remote_copy(
            src_ref=src,
            dst_ref=dst,
            send_sem=hsend_sem.at[i],
            recv_sem=hrecv_sem.at[i],
            device_id={"sp": following, "tp": 1 - tp},
            device_id_type=MESH,
        )
        for i, (src, dst) in enumerate(
            (
                (KA.at[tail, :], KH.at[1]),
                (KB.at[tail, :], KH.at[0]),
                (VA.at[:, tail], VH.at[1]),
                (VB.at[:, tail], VH.at[0]),
                (PA.at[rows - HALO : rows], PH.at[1]),
                (PB.at[rows - HALO : rows], PH.at[0]),
            )
        )
    ]

    def total_copy(place, core, source):
        return pltpu.make_async_remote_copy(
            src_ref=TOT,
            dst_ref=RECV.at[source],
            send_sem=tsend_sem.at[place * 2 + core],
            recv_sem=trecv_sem.at[source],
            device_id={"sp": place, "tp": core},
            device_id_type=MESH,
        )

    def for_later(act):
        @pl.when(tp == 0)
        def _():
            act(sp, 1)

        @pl.loop(sp + 1, sp_count)
        def _(place):
            act(place, 0)
            act(place, 1)

    def send_out():
        pl.semaphore_wait(barrier, count - 1)

        @pl.when(jnp.logical_not(last))
        def _():
            for copy in halo_copies:
                copy.start()

        for_later(lambda place, core: total_copy(place, core, me).start())

    pairs = 2 * BLK
    older = lax.broadcasted_iota(jnp.int32, (BLK, pairs), 0) > (
        lax.broadcasted_iota(jnp.int32, (BLK, pairs), 1) & (BLK - 1)
    )
    KEEP[0] = jnp.where(older, 1.0, 0.0).astype(BF16)
    KEEP[1] = jnp.where(older, 0.0, 1.0).astype(BF16)
    per_kv = QUERY_HEADS // KEY_VALUE_HEADS

    def query_rows(h, ahead):
        source, row = (QA, h) if h < own_heads else (QB, h - own_heads)
        return source[row * HEAD_SIZE : (row + 1) * HEAD_SIZE, ahead]

    kv_side = KEY_VALUE_HEADS // 2

    def attend(*spec):
        units = []
        for b, hide in spec:
            start = pl.multiple_of(b * BLK, BLK)
            for h in range(0, QUERY_HEADS, 2):
                units.append((start, hide, h))
        parts = {}

        def ask(index):
            start, hide, h = units[index]
            ahead = pl.ds(start, BLK)
            both = pl.ds(pl.multiple_of(start - BLK, BLK), 2 * BLK)
            side, slot = divmod(h // per_kv, kv_side)
            keys, values = (KA, VA) if side == 0 else (KB, VB)
            at_head = slice(slot * HEAD_SIZE, (slot + 1) * HEAD_SIZE)
            if hide is None:
                key_part, value_part = keys[both, at_head], values[at_head, both]
            else:
                key_part = jnp.concatenate([KH[side, :, at_head], keys[0:BLK, at_head]], axis=0)
                value_part = jnp.concatenate([VH[side, at_head, :], values[at_head, 0:BLK]], axis=1)
            query_part = jnp.concatenate([query_rows(h, ahead), query_rows(h + 1, ahead)], axis=1)
            sink = jnp.concatenate([SK[h : h + 1, :], SK[h + 1 : h + 2, :]], axis=1)
            score = jnp.dot(key_part, query_part, preferred_element_type=F32)
            parts[index] = (ahead, hide, h, score, value_part, sink)

        for index in range(min(AHEAD, len(units))):
            ask(index)
        results = []
        for index in range(len(units)):
            ahead, hide, h, score, value_part, sink = parts.pop(index)
            before = score[:BLK]
            if hide is not None:
                before = before + hide
            merged = jnp.where(older, before, score[BLK:])
            row_max = jnp.maximum(jnp.max(merged, axis=0, keepdims=True), sink)
            weights = jnp.exp(merged - row_max)
            weight_sum = jnp.sum(weights, axis=0, keepdims=True) + jnp.exp(sink - row_max)
            rounded = weights.astype(BF16)
            if index + AHEAD < len(units):
                ask(index + AHEAD)
            spread = jnp.concatenate([rounded * KEEP[0], rounded * KEEP[1]], axis=0)
            mixed = jnp.dot(value_part, spread, preferred_element_type=F32)
            mixed = mixed * (1.0 / weight_sum)
            stacked = jnp.concatenate([mixed[:, :BLK], mixed[:, BLK:]], axis=0).astype(BF16)
            results.append((ahead, h, stacked.T, row_max + jnp.log(weight_sum)))
        for ahead, h, out, logs in results:
            LS[h : h + 1, ahead] = logs[:, :BLK]
            LS[h + 1 : h + 2, ahead] = logs[:, BLK:]
            column = lax.rem(tp * half_q + h * HEAD_SIZE, qw)
            ATT[ahead, pl.ds(pl.multiple_of(column, 128), 2 * HEAD_SIZE)] = out

    def share(first_row, last_row):
        for n in range(0, PART.shape[1], OUT_TILE):
            PART[first_row:last_row, n : n + OUT_TILE] = jnp.dot(
                ATT[first_row:last_row, :], WOA[:, n : n + OUT_TILE], preferred_element_type=F32
            )

    @pl.loop(1, blocks // 2)
    def _(b):
        @pl.when(b == SEND_STEP)
        def _():
            send_out()

        attend((2 * b, None), (2 * b + 1, None))

    for copy in out_copies:
        copy.wait()
    share(2 * BLK, rows)

    @pl.when(jnp.logical_not(first))
    def _():
        for copy in halo_copies:
            copy.wait_recv()

    attend((1, None), (0, jnp.where(first, -jnp.inf, 0.0).astype(F32)))

    mine = pl.ds(pl.multiple_of(tp * rows, 128), rows)
    log_swap = pltpu.make_async_remote_copy(
        src_ref=LS.at[own_heads : 2 * own_heads, :],
        dst_ref=LSR.at[:, mine],
        send_sem=lsend_sem,
        recv_sem=lrecv_sem,
        device_id={"tp": 1 - tp},
        device_id_type=MESH,
    )
    log_swap.start()
    LSR[:, mine] = LS[0:own_heads, :]

    share(0, 2 * BLK)

    @pl.loop(0, sp)
    def _(place):
        total_copy(place, 0, place * 2).wait_recv()
        total_copy(place, 1, place * 2 + 1).wait_recv()

    @pl.when(tp == 1)
    def _():
        total_copy(sp, 0, sp * 2).wait_recv()

    earlier = jnp.zeros(EARLIER.shape, F32)
    for source in range(count - 1):
        earlier += jnp.where(source < me, RECV[source], 0.0)
    EARLIER[...] = earlier

    log_swap.wait()

    @pl.when(jnp.logical_not(last))
    def _():
        for copy in halo_copies:
            copy.wait_send()

    for_later(lambda place, core: total_copy(place, core, me).wait_send())


def output_kernel(
    PA,
    PB,
    PH,
    before,
    WG,
    WOP,
    PART,
    logs,
    mixed_out,
    logs_out,
    POOL,
    MIXED,
    EARLIER,
    BAND,
    out_sem,
    log_sem,
):
    rows, half_p = PA.shape
    width = MIXED.shape[1]
    blocks = rows // BLK
    tp = lax.axis_index("tp")
    me = lax.axis_index("sp") * 2 + tp
    log_copy = pltpu.make_async_copy(logs, logs_out, log_sem)
    log_copy.start()

    span = HALO + BLK
    back = (
        lax.broadcasted_iota(jnp.int32, (BLK, span), 0)
        + HALO
        - lax.broadcasted_iota(jnp.int32, (BLK, span), 1)
    )
    in_block = lax.broadcasted_iota(jnp.int32, (BLK, span), 1) >= HALO
    prefix_ones = jnp.where((back >= 0) & in_block, 1.0, 0.0).astype(BF16)
    groups = [lax.rem(2 * tp + j, GROUPS) for j in range(GROUPS)]
    reaches = [jnp.left_shift(jnp.int32(2), group) for group in groups]
    for j, reach in enumerate(reaches):
        BAND[j, 0:BLK, :] = jnp.where(
            (back >= 0) & (back < reach), 1.0 / reach.astype(F32), 0.0
        ).astype(BF16)
        BAND[j, BLK : 2 * BLK, :] = prefix_ones

    EARLIER[...] = before[...]
    local_row = lax.broadcasted_iota(jnp.int32, (BLK, 128), 0)
    pair = 2 * BLK

    def pair_rows(index):
        return pl.ds(pl.multiple_of(index * pair, pair), pair)

    def out_copy(index):
        at = pair_rows(index)
        return pltpu.make_async_copy(MIXED.at[at], mixed_out.at[at], out_sem.at[index])

    def step(done, spec):
        units = []
        for b, opening in spec:
            start = pl.multiple_of(b * BLK, BLK)
            for j in range(GROUPS):
                side, at_group = j // 2, slice((j % 2) * GDIM, (j % 2 + 1) * GDIM)
                held = PA if side == 0 else PB
                if opening:
                    source = jnp.concatenate([PH[side, :, at_group], held[0:BLK, at_group]], axis=0)
                else:
                    source = held[pl.ds(pl.multiple_of(start - HALO, HALO), span), at_group]
                units.append((b, opening, j, source))
        sides = [pl.ds(tp if j < 2 else 1 - tp, 1) for j in range(GROUPS)]
        carries = [
            EARLIER[sides[j], 0, (j % 2) * GDIM : (j % 2 + 1) * GDIM] for j in range(GROUPS)
        ]
        sums = [
            jnp.dot(BAND[j], source, preferred_element_type=F32) for b, opening, j, source in units
        ]
        rates = {}
        for b, opening in spec:
            seen = (me * rows + b * BLK + 1 + local_row).astype(F32)
            rates[id(b)] = (seen, 1.0 / seen)
        outs, parts = [], []

        def pool_unit(index):
            b, opening, j, source = units[index]
            seen, per_seen = rates[id(b)]
            window_mean = sums[index][:BLK]
            if opening:
                reach = reaches[j].astype(F32)
                fewer = reach / jnp.minimum(seen, reach)
                window_mean = window_mean * jnp.concatenate([fewer, fewer], axis=1)
            prefix = sums[index][BLK:] + carries[j]
            carries[j] = prefix[BLK - 1 : BLK, :]
            rate = jnp.concatenate([per_seen, per_seen], axis=1)
            pooled = (window_mean - prefix * rate).astype(BF16)
            out = jnp.dot(pooled, WG[j], preferred_element_type=F32).astype(BF16)
            outs.append((pl.ds(pl.multiple_of(b * BLK, BLK), BLK), groups[j], out))

        tiles = range(0, width, GDIM) if done is not None else ()
        for index, n in enumerate(tiles):
            ready = jnp.dot(POOL[pair_rows(done), :], WOP[:, n : n + GDIM], preferred_element_type=F32)
            parts.append((n, (ready + PART[pair_rows(done), n : n + GDIM]).astype(BF16)))
            if index < len(units):
                pool_unit(index)
        for index in range(len(tiles), len(units)):
            pool_unit(index)
        for n, part in parts:
            MIXED[pair_rows(done), n : n + GDIM] = part
        if units:
            for j in range(GROUPS):
                EARLIER[sides[j], 0, (j % 2) * GDIM : (j % 2 + 1) * GDIM] = carries[j]
        for at, group, out in outs:
            POOL[at, pl.ds(pl.multiple_of(group * GDIM, GDIM), GDIM)] = out
        if done is not None:
            out_copy(done).start()

    step(None, ((0, True), (1, False)))

    @pl.loop(1, blocks // 2)
    def _(index):
        step(index - 1, ((2 * index, False), (2 * index + 1, False)))

    step(blocks // 2 - 1, ())
    for index in range(blocks // 2):
        out_copy(index).wait()
    log_copy.wait()


def body(sp_count, tokens, norm_gain, w_query, w_key, w_value, w_pool, w_group, w_out, sinks):
    token_rows = tokens[0]
    both_rows, width = token_rows.shape
    rows = both_rows // 2
    pw, qw, kw = 2 * w_pool.shape[1], 2 * w_query.shape[1], 2 * w_key.shape[1]
    count = sp_count * 2
    blocks = rows // BLK
    hbm = pl.BlockSpec(memory_space=pltpu.HBM)
    vmem = pl.BlockSpec(memory_space=pltpu.VMEM)
    dma = pltpu.SemaphoreType.DMA
    arguments = (
        token_rows,
        norm_gain[None, :],
        w_query,
        w_key,
        w_value,
        w_pool,
        w_group,
        sinks,
    )
    projected = pl.pallas_call(
        project_kernel,
        out_shape=(
            jax.ShapeDtypeStruct((rows, width), BF16),
            jax.ShapeDtypeStruct((width, pw // 2), BF16),
            jax.ShapeDtypeStruct((width, qw // 2), BF16),
            jax.ShapeDtypeStruct((width, kw), BF16),
            jax.ShapeDtypeStruct((GROUPS, GDIM, GDIM), BF16),
            jax.ShapeDtypeStruct((QUERY_HEADS, 128), F32),
            jax.ShapeDtypeStruct((rows, pw // 2), BF16),
            jax.ShapeDtypeStruct((qw // 2, rows), BF16),
            jax.ShapeDtypeStruct((rows, kw // 2), BF16),
            jax.ShapeDtypeStruct((kw // 2, rows), BF16),
            jax.ShapeDtypeStruct((1, pw // 2), F32),
        ),
        in_specs=[hbm] * 8,
        out_specs=(vmem,) * 11,
        scratch_shapes=[
            pltpu.VMEM((1, width), F32),
            pltpu.VMEM((8, width), F32),
            pltpu.SMEM((QUERY_HEADS // 2,), F32),
            pltpu.VMEM((width, pw // 2), BF16),
            pltpu.VMEM((width, qw // 2), BF16),
            pltpu.VMEM((width, kw), BF16),
            dma((blocks,)),
            dma((5,)),
            dma((2,)),
            dma((6,)),
            dma((6,)),
        ],
        compiler_params=pltpu.CompilerParams(
            collective_id=0, has_side_effects=True, vmem_limit_bytes=20 * 2**20
        ),
        name="project",
    )(*(pltpu.with_memory_space_constraint(array, pltpu.HBM) for array in arguments))

    part, logs, other_pool, pool_halo, earlier, pool_weights = pl.pallas_call(
        functools.partial(mixer_kernel, sp_count),
        out_shape=(
            jax.ShapeDtypeStruct((rows, w_out.shape[1]), F32),
            jax.ShapeDtypeStruct((QUERY_HEADS // 2, both_rows), F32),
            jax.ShapeDtypeStruct((rows, pw // 2), BF16),
            jax.ShapeDtypeStruct((2, HALO, pw // 2), BF16),
            jax.ShapeDtypeStruct((2, 1, pw // 2), F32),
            jax.ShapeDtypeStruct((pw, w_out.shape[1]), BF16),
        ),
        in_specs=[vmem] * 11 + [hbm],
        out_specs=(vmem,) * 6,
        scratch_shapes=[
            pltpu.VMEM((rows, qw), BF16),
            pltpu.VMEM((qw, w_out.shape[1]), BF16),
            pltpu.VMEM((qw // 2, rows), BF16),
            pltpu.VMEM((rows, kw // 2), BF16),
            pltpu.VMEM((kw // 2, rows), BF16),
            pltpu.VMEM((2, BLK, kw // 2), BF16),
            pltpu.VMEM((2, kw // 2, BLK), BF16),
            pltpu.VMEM((QUERY_HEADS, rows), F32),
            pltpu.VMEM((2, 1, pw // 2), F32),
            pltpu.VMEM((count, 2, 1, pw // 2), F32),
            pltpu.VMEM((2, BLK, 2 * BLK), BF16),
            dma((6,)),
            dma((6,)),
            dma((count,)),
            dma((count,)),
            dma,
            dma,
            dma((2,)),
        ],
        compiler_params=pltpu.CompilerParams(
            collective_id=1, has_side_effects=True, vmem_limit_bytes=20 * 2**20
        ),
        name="mixers",
    )(*projected, pltpu.with_memory_space_constraint(w_out, pltpu.HBM))

    mixed, log_sums = pl.pallas_call(
        output_kernel,
        out_shape=(
            jax.ShapeDtypeStruct((rows, w_out.shape[1]), BF16),
            jax.ShapeDtypeStruct((QUERY_HEADS // 2, both_rows), F32),
        ),
        in_specs=[vmem] * 8,
        out_specs=(hbm, hbm),
        scratch_shapes=[
            pltpu.VMEM((rows, pw), BF16),
            pltpu.VMEM((rows, w_out.shape[1]), BF16),
            pltpu.VMEM((2, 1, pw // 2), F32),
            pltpu.VMEM((GROUPS, 2 * BLK, HALO + BLK), BF16),
            dma((blocks // 2,)),
            dma,
        ],
        compiler_params=pltpu.CompilerParams(vmem_limit_bytes=24 * 2**20),
        name="output",
    )(
        projected[PA_INDEX],
        other_pool,
        pool_halo,
        earlier,
        projected[WG_INDEX],
        pool_weights,
        part,
        logs,
    )
    return mixed[None], log_sums[None]


def solution(mesh):
    return jax.shard_map(
        functools.partial(body, mesh.shape["sp"]),
        mesh=mesh,
        in_specs=(
            P("fs", "sp", None),
            P(),
            P(None, "tp"),
            P(None, "tp"),
            P(None, "tp"),
            P(None, "tp"),
            P("tp", None, None),
            P(),
            P("tp"),
        ),
        out_specs=(P("fs", ("sp", "tp"), None), P("fs", "tp", "sp")),
        check_vma=False,
    )
```

```python
import functools

import jax
import jax.numpy as jnp
from jax import lax
from jax.experimental import pallas as pl
from jax.experimental.pallas import tpu as pltpu
from jax.sharding import PartitionSpec as P

HEAD_SIZE = 64
GROUPS = 4
GDIM = 256
WINDOW_KEYS = 128
QUERY_HEADS = 16
KEY_VALUE_HEADS = 4
LN_EPS = 1e-05

BLK = 128
HALO = 16
TILE = 256
F32, BF16 = jnp.float32, jnp.bfloat16


MESH = pl.DeviceIdType.MESH
NORM_ROWS = 128
NORM_TILE = 256
OUT_TILE = 512
WG_INDEX, PA_INDEX = 4, 6
STEPS = (512,)
AHEAD = 8


def project_kernel(
    tok,
    gain,
    w_query,
    w_key,
    w_value,
    w_pool,
    w_group,
    sinks,
    X,
    WP,
    WQ,
    WKV,
    WG,
    SK,
    PA,
    QA,
    KA,
    VA,
    TA,
    GAIN,
    GAINS,
    SINK,
    WPO,
    WQO,
    WKVO,
    x_sem,
    w_sem,
    small_sem,
    send_sem,
    recv_sem,
):
    rows, width = X.shape
    blocks = rows // BLK
    half_p, half_q, half_k = PA.shape[1], QA.shape[0], KA.shape[1]
    own_heads = QUERY_HEADS // 2
    tp = lax.axis_index("tp")
    peer = {"tp": 1 - tp}

    barrier = pltpu.get_barrier_semaphore()
    pl.semaphore_signal(barrier, inc=1, device_id=peer, device_id_type=MESH)

    small = [
        pltpu.make_async_copy(gain, GAIN, small_sem.at[0]),
        pltpu.make_async_copy(sinks, SINK, small_sem.at[1]),
    ]
    for copy in small:
        copy.start()

    def x_copy(b):
        return pltpu.make_async_copy(
            tok.at[pl.ds(pl.multiple_of(tp * rows + b * BLK, BLK), BLK), :],
            X.at[b * BLK : (b + 1) * BLK, :],
            x_sem.at[b],
        )

    for b in range(blocks):
        x_copy(b).start()

    pl.semaphore_wait(barrier, 1)
    sends = [
        pltpu.make_async_remote_copy(
            src_ref=src,
            dst_ref=dst,
            send_sem=send_sem.at[i],
            recv_sem=recv_sem.at[i],
            device_id=peer,
            device_id_type=MESH,
        )
        for i, (src, dst) in enumerate(
            (
                (w_pool, WP),
                (w_key, WKV.at[:, 0:half_k]),
                (w_value, WKV.at[:, half_k : 2 * half_k]),
                (w_query, WQ),
                (w_group, WG.at[GROUPS // 2 : GROUPS]),
                (SK.at[0:own_heads], SK.at[own_heads : 2 * own_heads]),
            )
        )
    ]
    for copy in sends[:5]:
        copy.start()

    own = [
        pltpu.make_async_copy(src, dst, w_sem.at[i])
        for i, (src, dst) in enumerate(
            (
                (w_pool, WPO),
                (w_query, WQO),
                (w_key, WKVO.at[:, 0:half_k]),
                (w_value, WKVO.at[:, half_k : 2 * half_k]),
                (w_group, WG.at[0 : GROUPS // 2]),
            )
        )
    ]
    for copy in own:
        copy.start()

    for copy in small:
        copy.wait()
    row_of = lax.broadcasted_iota(jnp.int32, (own_heads, 128), 0)
    sink_block = jnp.zeros((own_heads, 128), F32)
    for h in range(own_heads):
        sink_block = jnp.where(row_of == h, SINK[h], sink_block)
    SK[0:own_heads, :] = sink_block

    GAINS[...] = jnp.broadcast_to(GAIN[...], GAINS.shape)

    def normalized(row):
        values = X[row : row + NORM_ROWS, :].astype(F32)
        mean = jnp.sum(values, axis=-1, keepdims=True) * (1.0 / width)
        centered = values - mean
        variance = jnp.sum(centered * centered, axis=-1, keepdims=True) * (1.0 / width)
        scaled = (centered * lax.rsqrt(variance + LN_EPS)).reshape(-1, 8, width)
        return (scaled * GAINS[...][None]).reshape(NORM_ROWS, width).astype(BF16)

    def project(first_row, last_row, normed_to):
        at = slice(first_row, last_row)
        todo = list(range(last_row, normed_to, NORM_ROWS))
        slots = (half_p + half_q) // NORM_TILE
        following, pools, queries = [], [], []
        rows_in = X[at, :]

        def norm_some(slot):
            for row in todo[len(todo) * slot // slots : len(todo) * (slot + 1) // slots]:
                following.append((row, normalized(row)))

        for n in range(0, half_p, NORM_TILE):
            pools.append(jnp.dot(rows_in, WPO[:, n : n + NORM_TILE], preferred_element_type=F32))
            norm_some(n // NORM_TILE)
        for n in range(0, half_q, NORM_TILE):
            queries.append(jnp.dot(rows_in, WQO[:, n : n + NORM_TILE], preferred_element_type=F32))
            norm_some((half_p + n) // NORM_TILE)
        both = jnp.dot(rows_in, WKVO[...], preferred_element_type=F32).astype(BF16)
        for row, block in following:
            X[row : row + NORM_ROWS, :] = block
        for index, pool in enumerate(pools):
            columns = slice(index * NORM_TILE, (index + 1) * NORM_TILE)
            rounded = pool.astype(BF16)
            PA[at, columns] = rounded
            total = jnp.sum(rounded.astype(F32), axis=0, keepdims=True)
            TA[:, columns] = total if first_row == 0 else TA[:, columns] + total
        for index, query in enumerate(queries):
            at_rows = slice(index * NORM_TILE, (index + 1) * NORM_TILE)
            QA[at_rows, at] = (query * (HEAD_SIZE**-0.5)).astype(BF16).T
        KA[at, :] = both[:, :half_k]
        VA[:, at] = both[:, half_k:].T

    for row in range(0, STEPS[0], NORM_ROWS):
        x_copy(row // BLK).wait()
        X[row : row + NORM_ROWS, :] = normalized(row)
    for b in range(STEPS[0] // BLK, blocks):
        x_copy(b).wait()
    sends[5].start()
    for copy in own:
        copy.wait()
    bounds = (0, *STEPS, rows, rows)
    for step in range(len(bounds) - 2):
        project(*bounds[step : step + 3])

    for copy in sends:
        copy.wait()


def mixer_kernel(
    sp_count,
    X,
    WP,
    WQ,
    WKV,
    WG,
    SK,
    PA,
    QA,
    KA,
    VA,
    TA,
    w_out,
    PART,
    LSR,
    PB,
    PH,
    EARLIER,
    WOP,
    ATT,
    WOA,
    QB,
    KB,
    VB,
    KH,
    VH,
    LS,
    TOT,
    RECV,
    KEEP,
    hsend_sem,
    hrecv_sem,
    tsend_sem,
    trecv_sem,
    lsend_sem,
    lrecv_sem,
    out_sem,
):
    rows, half_k = KB.shape
    half_p, half_q = PA.shape[1], QA.shape[0]
    pw, qw = 2 * half_p, 2 * half_q
    blocks = rows // BLK
    sp, tp = lax.axis_index("sp"), lax.axis_index("tp")
    me = sp * 2 + tp
    count = sp_count * 2
    own_heads = QUERY_HEADS // 2
    first, last = me == 0, me == count - 1

    out_copies = [
        pltpu.make_async_copy(w_out.at[pw : pw + qw], WOA, out_sem.at[0]),
        pltpu.make_async_copy(w_out.at[0:pw], WOP, out_sem.at[1]),
    ]
    for copy in out_copies:
        copy.start()

    barrier = pltpu.get_barrier_semaphore()

    def arrive(device):
        pl.semaphore_signal(barrier, inc=1, device_id=device, device_id_type=MESH)

    arrive({"tp": 1 - tp})
    for distance in range(1, sp_count):
        place = sp + distance
        place = jnp.where(place >= sp_count, place - sp_count, place)
        for core in range(2):
            arrive({"sp": place, "tp": core})

    @pl.when(first)
    def _():
        PH[...] = jnp.zeros_like(PH)
        KH[...] = jnp.zeros_like(KH)
        VH[...] = jnp.zeros_like(VH)

    tile = jnp.dot(X[...], WP[...], preferred_element_type=F32).astype(BF16)
    PB[...] = tile
    TOT[pl.ds(tp, 1), 0] = TA[...]
    TOT[pl.ds(1 - tp, 1), 0] = jnp.sum(tile.astype(F32), axis=0, keepdims=True)
    tile = jnp.dot(X[...], WKV[...], preferred_element_type=F32).astype(BF16)
    KB[...] = tile[:, :half_k]
    VB[...] = tile[:, half_k:].T
    tile = jnp.dot(X[...], WQ[...], preferred_element_type=F32) * (HEAD_SIZE**-0.5)
    QB[...] = tile.astype(BF16).T

    tail = slice(rows - BLK, rows)
    following = lax.rem(sp + tp, sp_count)
    halo_copies = [
        pltpu.make_async_remote_copy(
            src_ref=src,
            dst_ref=dst,
            send_sem=hsend_sem.at[i],
            recv_sem=hrecv_sem.at[i],
            device_id={"sp": following, "tp": 1 - tp},
            device_id_type=MESH,
        )
        for i, (src, dst) in enumerate(
            (
                (KA.at[tail, :], KH.at[1]),
                (KB.at[tail, :], KH.at[0]),
                (VA.at[:, tail], VH.at[1]),
                (VB.at[:, tail], VH.at[0]),
                (PA.at[rows - HALO : rows], PH.at[1]),
                (PB.at[rows - HALO : rows], PH.at[0]),
            )
        )
    ]

    def total_copy(place, core, source):
        return pltpu.make_async_remote_copy(
            src_ref=TOT,
            dst_ref=RECV.at[source],
            send_sem=tsend_sem.at[place * 2 + core],
            recv_sem=trecv_sem.at[source],
            device_id={"sp": place, "tp": core},
            device_id_type=MESH,
        )

    def for_later(act):
        @pl.when(tp == 0)
        def _():
            act(sp, 1)

        @pl.loop(sp + 1, sp_count)
        def _(place):
            act(place, 0)
            act(place, 1)

    def send_out():
        pl.semaphore_wait(barrier, count - 1)

        @pl.when(jnp.logical_not(last))
        def _():
            for copy in halo_copies:
                copy.start()

        for_later(lambda place, core: total_copy(place, core, me).start())

    pairs = 2 * BLK
    older = lax.broadcasted_iota(jnp.int32, (BLK, pairs), 0) > (
        lax.broadcasted_iota(jnp.int32, (BLK, pairs), 1) & (BLK - 1)
    )
    KEEP[0] = jnp.where(older, 1.0, 0.0).astype(BF16)
    KEEP[1] = jnp.where(older, 0.0, 1.0).astype(BF16)
    per_kv = QUERY_HEADS // KEY_VALUE_HEADS

    def query_rows(h, ahead):
        source, row = (QA, h) if h < own_heads else (QB, h - own_heads)
        return source[row * HEAD_SIZE : (row + 1) * HEAD_SIZE, ahead]

    kv_side = KEY_VALUE_HEADS // 2

    def attend(*spec, done=None):
        ready = []
        if done is not None:
            at = pl.ds(pl.multiple_of(done * 2 * BLK, 2 * BLK), 2 * BLK)
            attended = ATT[at, :]
        units = []
        for b, hide in spec:
            start = pl.multiple_of(b * BLK, BLK)
            for h in range(0, QUERY_HEADS, 2):
                units.append((start, hide, h))
        parts = {}

        def ask(index):
            start, hide, h = units[index]
            ahead = pl.ds(start, BLK)
            both = pl.ds(pl.multiple_of(start - BLK, BLK), 2 * BLK)
            side, slot = divmod(h // per_kv, kv_side)
            keys, values = (KA, VA) if side == 0 else (KB, VB)
            at_head = slice(slot * HEAD_SIZE, (slot + 1) * HEAD_SIZE)
            if hide is None:
                key_part, value_part = keys[both, at_head], values[at_head, both]
            else:
                key_part = jnp.concatenate([KH[side, :, at_head], keys[0:BLK, at_head]], axis=0)
                value_part = jnp.concatenate([VH[side, at_head, :], values[at_head, 0:BLK]], axis=1)
            query_part = jnp.concatenate([query_rows(h, ahead), query_rows(h + 1, ahead)], axis=1)
            sink = jnp.concatenate([SK[h : h + 1, :], SK[h + 1 : h + 2, :]], axis=1)
            score = jnp.dot(key_part, query_part, preferred_element_type=F32)
            parts[index] = (ahead, hide, h, score, value_part, sink)

        for index in range(min(AHEAD, len(units))):
            ask(index)
        results = []
        for index in range(len(units)):
            ahead, hide, h, score, value_part, sink = parts.pop(index)
            if done is not None and index % 2 == 0:
                n = (index // 2) * GDIM
                ready.append(
                    jnp.dot(attended, WOA[:, n : n + GDIM], preferred_element_type=F32)
                )
            before = score[:BLK]
            if hide is not None:
                before = before + hide
            merged = jnp.where(older, before, score[BLK:])
            row_max = jnp.maximum(jnp.max(merged, axis=0, keepdims=True), sink)
            weights = jnp.exp(merged - row_max)
            weight_sum = jnp.sum(weights, axis=0, keepdims=True) + jnp.exp(sink - row_max)
            rounded = weights.astype(BF16)
            if index + AHEAD < len(units):
                ask(index + AHEAD)
            spread = jnp.concatenate([rounded * KEEP[0], rounded * KEEP[1]], axis=0)
            mixed = jnp.dot(value_part, spread, preferred_element_type=F32)
            mixed = mixed * (1.0 / weight_sum)
            stacked = jnp.concatenate([mixed[:, :BLK], mixed[:, BLK:]], axis=0).astype(BF16)
            results.append((ahead, h, stacked.T, row_max + jnp.log(weight_sum)))
        for n, part in enumerate(ready):
            PART[at, n * GDIM : (n + 1) * GDIM] = part
        for ahead, h, out, logs in results:
            LS[h : h + 1, ahead] = logs[:, :BLK]
            LS[h + 1 : h + 2, ahead] = logs[:, BLK:]
            column = lax.rem(tp * half_q + h * HEAD_SIZE, qw)
            ATT[ahead, pl.ds(pl.multiple_of(column, 128), 2 * HEAD_SIZE)] = out

    def share(first_row, last_row):
        for n in range(0, PART.shape[1], OUT_TILE):
            PART[first_row:last_row, n : n + OUT_TILE] = jnp.dot(
                ATT[first_row:last_row, :], WOA[:, n : n + OUT_TILE], preferred_element_type=F32
            )

    @pl.when(me >= 0)
    def _():
        attend((2, None), (3, None))

    send_out()
    for copy in out_copies:
        copy.wait()

    @pl.loop(2, blocks // 2)
    def _(b):
        attend((2 * b, None), (2 * b + 1, None), done=b - 1)

    @pl.when(jnp.logical_not(first))
    def _():
        for copy in halo_copies:
            copy.wait_recv()

    attend((1, None), (0, jnp.where(first, -jnp.inf, 0.0).astype(F32)), done=blocks // 2 - 1)

    mine = pl.ds(pl.multiple_of(tp * rows, 128), rows)
    log_swap = pltpu.make_async_remote_copy(
        src_ref=LS.at[own_heads : 2 * own_heads, :],
        dst_ref=LSR.at[:, mine],
        send_sem=lsend_sem,
        recv_sem=lrecv_sem,
        device_id={"tp": 1 - tp},
        device_id_type=MESH,
    )
    log_swap.start()
    LSR[:, mine] = LS[0:own_heads, :]

    share(0, 2 * BLK)

    @pl.loop(0, sp)
    def _(place):
        total_copy(place, 0, place * 2).wait_recv()
        total_copy(place, 1, place * 2 + 1).wait_recv()

    @pl.when(tp == 1)
    def _():
        total_copy(sp, 0, sp * 2).wait_recv()

    earlier = jnp.zeros(EARLIER.shape, F32)
    for source in range(count - 1):
        earlier += jnp.where(source < me, RECV[source], 0.0)
    EARLIER[...] = earlier

    log_swap.wait()

    @pl.when(jnp.logical_not(last))
    def _():
        for copy in halo_copies:
            copy.wait_send()

    for_later(lambda place, core: total_copy(place, core, me).wait_send())


def output_kernel(
    PA,
    PB,
    PH,
    before,
    WG,
    WOP,
    PART,
    logs,
    mixed_out,
    logs_out,
    POOL,
    MIXED,
    EARLIER,
    BAND,
    out_sem,
    log_sem,
):
    rows, half_p = PA.shape
    width = MIXED.shape[1]
    blocks = rows // BLK
    tp = lax.axis_index("tp")
    me = lax.axis_index("sp") * 2 + tp
    log_copy = pltpu.make_async_copy(logs, logs_out, log_sem)
    log_copy.start()

    span = HALO + BLK
    back = (
        lax.broadcasted_iota(jnp.int32, (BLK, span), 0)
        + HALO
        - lax.broadcasted_iota(jnp.int32, (BLK, span), 1)
    )
    in_block = lax.broadcasted_iota(jnp.int32, (BLK, span), 1) >= HALO
    prefix_ones = jnp.where((back >= 0) & in_block, 1.0, 0.0).astype(BF16)
    groups = [lax.rem(2 * tp + j, GROUPS) for j in range(GROUPS)]
    reaches = [jnp.left_shift(jnp.int32(2), group) for group in groups]
    for j, reach in enumerate(reaches):
        BAND[j, 0:BLK, :] = jnp.where(
            (back >= 0) & (back < reach), 1.0 / reach.astype(F32), 0.0
        ).astype(BF16)
        BAND[j, BLK : 2 * BLK, :] = prefix_ones

    EARLIER[...] = before[...]
    local_row = lax.broadcasted_iota(jnp.int32, (BLK, 128), 0)
    pair = 2 * BLK

    def pair_rows(index):
        return pl.ds(pl.multiple_of(index * pair, pair), pair)

    def out_copy(index):
        at = pair_rows(index)
        return pltpu.make_async_copy(MIXED.at[at], mixed_out.at[at], out_sem.at[index])

    def step(done, spec):
        units = []
        for b, opening in spec:
            start = pl.multiple_of(b * BLK, BLK)
            for j in range(GROUPS):
                side, at_group = j // 2, slice((j % 2) * GDIM, (j % 2 + 1) * GDIM)
                held = PA if side == 0 else PB
                if opening:
                    source = jnp.concatenate([PH[side, :, at_group], held[0:BLK, at_group]], axis=0)
                else:
                    source = held[pl.ds(pl.multiple_of(start - HALO, HALO), span), at_group]
                units.append((b, opening, j, source))
        sides = [pl.ds(tp if j < 2 else 1 - tp, 1) for j in range(GROUPS)]
        carries = [
            EARLIER[sides[j], 0, (j % 2) * GDIM : (j % 2 + 1) * GDIM] for j in range(GROUPS)
        ]
        sums = [
            jnp.dot(BAND[j], source, preferred_element_type=F32) for b, opening, j, source in units
        ]
        rates = {}
        for b, opening in spec:
            seen = (me * rows + b * BLK + 1 + local_row).astype(F32)
            rates[id(b)] = (seen, 1.0 / seen)
        outs, parts = [], []

        def pool_unit(index):
            b, opening, j, source = units[index]
            seen, per_seen = rates[id(b)]
            window_mean = sums[index][:BLK]
            if opening:
                reach = reaches[j].astype(F32)
                fewer = reach / jnp.minimum(seen, reach)
                window_mean = window_mean * jnp.concatenate([fewer, fewer], axis=1)
            prefix = sums[index][BLK:] + carries[j]
            carries[j] = prefix[BLK - 1 : BLK, :]
            rate = jnp.concatenate([per_seen, per_seen], axis=1)
            pooled = (window_mean - prefix * rate).astype(BF16)
            out = jnp.dot(pooled, WG[j], preferred_element_type=F32).astype(BF16)
            outs.append((pl.ds(pl.multiple_of(b * BLK, BLK), BLK), groups[j], out))

        tiles = range(0, width, GDIM) if done is not None else ()
        for index, n in enumerate(tiles):
            ready = jnp.dot(POOL[pair_rows(done), :], WOP[:, n : n + GDIM], preferred_element_type=F32)
            parts.append((n, (ready + PART[pair_rows(done), n : n + GDIM]).astype(BF16)))
            if index < len(units):
                pool_unit(index)
        for index in range(len(tiles), len(units)):
            pool_unit(index)
        for n, part in parts:
            MIXED[pair_rows(done), n : n + GDIM] = part
        if units:
            for j in range(GROUPS):
                EARLIER[sides[j], 0, (j % 2) * GDIM : (j % 2 + 1) * GDIM] = carries[j]
        for at, group, out in outs:
            POOL[at, pl.ds(pl.multiple_of(group * GDIM, GDIM), GDIM)] = out
        if done is not None:
            out_copy(done).start()

    step(None, ((0, True), (1, False)))

    @pl.loop(1, blocks // 2)
    def _(index):
        step(index - 1, ((2 * index, False), (2 * index + 1, False)))

    step(blocks // 2 - 1, ())
    for index in range(blocks // 2):
        out_copy(index).wait()
    log_copy.wait()


def body(sp_count, tokens, norm_gain, w_query, w_key, w_value, w_pool, w_group, w_out, sinks):
    token_rows = tokens[0]
    both_rows, width = token_rows.shape
    rows = both_rows // 2
    pw, qw, kw = 2 * w_pool.shape[1], 2 * w_query.shape[1], 2 * w_key.shape[1]
    count = sp_count * 2
    blocks = rows // BLK
    hbm = pl.BlockSpec(memory_space=pltpu.HBM)
    vmem = pl.BlockSpec(memory_space=pltpu.VMEM)
    dma = pltpu.SemaphoreType.DMA
    arguments = (
        token_rows,
        norm_gain[None, :],
        w_query,
        w_key,
        w_value,
        w_pool,
        w_group,
        sinks,
    )
    projected = pl.pallas_call(
        project_kernel,
        out_shape=(
            jax.ShapeDtypeStruct((rows, width), BF16),
            jax.ShapeDtypeStruct((width, pw // 2), BF16),
            jax.ShapeDtypeStruct((width, qw // 2), BF16),
            jax.ShapeDtypeStruct((width, kw), BF16),
            jax.ShapeDtypeStruct((GROUPS, GDIM, GDIM), BF16),
            jax.ShapeDtypeStruct((QUERY_HEADS, 128), F32),
            jax.ShapeDtypeStruct((rows, pw // 2), BF16),
            jax.ShapeDtypeStruct((qw // 2, rows), BF16),
            jax.ShapeDtypeStruct((rows, kw // 2), BF16),
            jax.ShapeDtypeStruct((kw // 2, rows), BF16),
            jax.ShapeDtypeStruct((1, pw // 2), F32),
        ),
        in_specs=[hbm] * 8,
        out_specs=(vmem,) * 11,
        scratch_shapes=[
            pltpu.VMEM((1, width), F32),
            pltpu.VMEM((8, width), F32),
            pltpu.SMEM((QUERY_HEADS // 2,), F32),
            pltpu.VMEM((width, pw // 2), BF16),
            pltpu.VMEM((width, qw // 2), BF16),
            pltpu.VMEM((width, kw), BF16),
            dma((blocks,)),
            dma((5,)),
            dma((2,)),
            dma((6,)),
            dma((6,)),
        ],
        compiler_params=pltpu.CompilerParams(
            collective_id=0, has_side_effects=True, vmem_limit_bytes=20 * 2**20
        ),
        name="project",
    )(*(pltpu.with_memory_space_constraint(array, pltpu.HBM) for array in arguments))

    part, logs, other_pool, pool_halo, earlier, pool_weights = pl.pallas_call(
        functools.partial(mixer_kernel, sp_count),
        out_shape=(
            jax.ShapeDtypeStruct((rows, w_out.shape[1]), F32),
            jax.ShapeDtypeStruct((QUERY_HEADS // 2, both_rows), F32),
            jax.ShapeDtypeStruct((rows, pw // 2), BF16),
            jax.ShapeDtypeStruct((2, HALO, pw // 2), BF16),
            jax.ShapeDtypeStruct((2, 1, pw // 2), F32),
            jax.ShapeDtypeStruct((pw, w_out.shape[1]), BF16),
        ),
        in_specs=[vmem] * 11 + [hbm],
        out_specs=(vmem,) * 6,
        scratch_shapes=[
            pltpu.VMEM((rows, qw), BF16),
            pltpu.VMEM((qw, w_out.shape[1]), BF16),
            pltpu.VMEM((qw // 2, rows), BF16),
            pltpu.VMEM((rows, kw // 2), BF16),
            pltpu.VMEM((kw // 2, rows), BF16),
            pltpu.VMEM((2, BLK, kw // 2), BF16),
            pltpu.VMEM((2, kw // 2, BLK), BF16),
            pltpu.VMEM((QUERY_HEADS, rows), F32),
            pltpu.VMEM((2, 1, pw // 2), F32),
            pltpu.VMEM((count, 2, 1, pw // 2), F32),
            pltpu.VMEM((2, BLK, 2 * BLK), BF16),
            dma((6,)),
            dma((6,)),
            dma((count,)),
            dma((count,)),
            dma,
            dma,
            dma((2,)),
        ],
        compiler_params=pltpu.CompilerParams(
            collective_id=1, has_side_effects=True, vmem_limit_bytes=20 * 2**20
        ),
        name="mixers",
    )(*projected, pltpu.with_memory_space_constraint(w_out, pltpu.HBM))

    mixed, log_sums = pl.pallas_call(
        output_kernel,
        out_shape=(
            jax.ShapeDtypeStruct((rows, w_out.shape[1]), BF16),
            jax.ShapeDtypeStruct((QUERY_HEADS // 2, both_rows), F32),
        ),
        in_specs=[vmem] * 8,
        out_specs=(hbm, hbm),
        scratch_shapes=[
            pltpu.VMEM((rows, pw), BF16),
            pltpu.VMEM((rows, w_out.shape[1]), BF16),
            pltpu.VMEM((2, 1, pw // 2), F32),
            pltpu.VMEM((GROUPS, 2 * BLK, HALO + BLK), BF16),
            dma((blocks // 2,)),
            dma,
        ],
        compiler_params=pltpu.CompilerParams(vmem_limit_bytes=24 * 2**20),
        name="output",
    )(
        projected[PA_INDEX],
        other_pool,
        pool_halo,
        earlier,
        projected[WG_INDEX],
        pool_weights,
        part,
        logs,
    )
    return mixed[None], log_sums[None]


def solution(mesh):
    return jax.shard_map(
        functools.partial(body, mesh.shape["sp"]),
        mesh=mesh,
        in_specs=(
            P("fs", "sp", None),
            P(),
            P(None, "tp"),
            P(None, "tp"),
            P(None, "tp"),
            P(None, "tp"),
            P("tp", None, None),
            P(),
            P("tp"),
        ),
        out_specs=(P("fs", ("sp", "tp"), None), P("fs", "tp", "sp")),
        check_vma=False,
    )
```

```python
import functools

import jax
import jax.numpy as jnp
from jax import lax
from jax.experimental import pallas as pl
from jax.experimental.pallas import tpu as pltpu
from jax.sharding import PartitionSpec as P

HEAD_SIZE = 64
GROUPS = 4
GDIM = 256
WINDOW_KEYS = 128
QUERY_HEADS = 16
KEY_VALUE_HEADS = 4
LN_EPS = 1e-05

BLK = 128
HALO = 16
TILE = 256
F32, BF16 = jnp.float32, jnp.bfloat16


MESH = pl.DeviceIdType.MESH
NORM_ROWS = 128
NORM_TILE = 256
OUT_TILE = 512
WG_INDEX, PA_INDEX = 4, 6
STEPS = (640,)
AHEAD = 8


def project_kernel(
    tok,
    gain,
    w_query,
    w_key,
    w_value,
    w_pool,
    w_group,
    sinks,
    X,
    WP,
    WQ,
    WKV,
    WG,
    SK,
    PA,
    QA,
    KA,
    VA,
    TA,
    GAIN,
    GAINS,
    SINK,
    WPO,
    WQO,
    WKVO,
    x_sem,
    w_sem,
    small_sem,
    send_sem,
    recv_sem,
):
    rows, width = X.shape
    blocks = rows // BLK
    half_p, half_q, half_k = PA.shape[1], QA.shape[0], KA.shape[1]
    own_heads = QUERY_HEADS // 2
    tp = lax.axis_index("tp")
    peer = {"tp": 1 - tp}

    barrier = pltpu.get_barrier_semaphore()
    pl.semaphore_signal(barrier, inc=1, device_id=peer, device_id_type=MESH)

    small = [
        pltpu.make_async_copy(gain, GAIN, small_sem.at[0]),
        pltpu.make_async_copy(sinks, SINK, small_sem.at[1]),
    ]
    for copy in small:
        copy.start()

    def x_copy(b):
        return pltpu.make_async_copy(
            tok.at[pl.ds(pl.multiple_of(tp * rows + b * BLK, BLK), BLK), :],
            X.at[b * BLK : (b + 1) * BLK, :],
            x_sem.at[b],
        )

    for b in range(blocks):
        x_copy(b).start()

    pl.semaphore_wait(barrier, 1)
    sends = [
        pltpu.make_async_remote_copy(
            src_ref=src,
            dst_ref=dst,
            send_sem=send_sem.at[i],
            recv_sem=recv_sem.at[i],
            device_id=peer,
            device_id_type=MESH,
        )
        for i, (src, dst) in enumerate(
            (
                (w_pool, WP),
                (w_key, WKV.at[:, 0:half_k]),
                (w_value, WKV.at[:, half_k : 2 * half_k]),
                (w_query, WQ),
                (w_group, WG.at[GROUPS // 2 : GROUPS]),
                (SK.at[0:own_heads], SK.at[own_heads : 2 * own_heads]),
            )
        )
    ]
    for copy in sends[:5]:
        copy.start()

    own = [
        pltpu.make_async_copy(src, dst, w_sem.at[i])
        for i, (src, dst) in enumerate(
            (
                (w_pool, WPO),
                (w_query, WQO),
                (w_key, WKVO.at[:, 0:half_k]),
                (w_value, WKVO.at[:, half_k : 2 * half_k]),
                (w_group, WG.at[0 : GROUPS // 2]),
            )
        )
    ]
    for copy in own:
        copy.start()

    for copy in small:
        copy.wait()
    row_of = lax.broadcasted_iota(jnp.int32, (own_heads, 128), 0)
    sink_block = jnp.zeros((own_heads, 128), F32)
    for h in range(own_heads):
        sink_block = jnp.where(row_of == h, SINK[h], sink_block)
    SK[0:own_heads, :] = sink_block

    GAINS[...] = jnp.broadcast_to(GAIN[...], GAINS.shape)

    def normalized(row):
        values = X[row : row + NORM_ROWS, :].astype(F32)
        mean = jnp.sum(values, axis=-1, keepdims=True) * (1.0 / width)
        centered = values - mean
        variance = jnp.sum(centered * centered, axis=-1, keepdims=True) * (1.0 / width)
        scaled = (centered * lax.rsqrt(variance + LN_EPS)).reshape(-1, 8, width)
        return (scaled * GAINS[...][None]).reshape(NORM_ROWS, width).astype(BF16)

    def project(first_row, last_row, normed_to):
        at = slice(first_row, last_row)
        todo = list(range(last_row, normed_to, NORM_ROWS))
        slots = (half_p + half_q) // NORM_TILE
        following, pools, queries = [], [], []
        rows_in = X[at, :]

        def norm_some(slot):
            for row in todo[len(todo) * slot // slots : len(todo) * (slot + 1) // slots]:
                following.append((row, normalized(row)))

        for n in range(0, half_p, NORM_TILE):
            pools.append(jnp.dot(rows_in, WPO[:, n : n + NORM_TILE], preferred_element_type=F32))
            norm_some(n // NORM_TILE)
        for n in range(0, half_q, NORM_TILE):
            queries.append(jnp.dot(rows_in, WQO[:, n : n + NORM_TILE], preferred_element_type=F32))
            norm_some((half_p + n) // NORM_TILE)
        both = jnp.dot(rows_in, WKVO[...], preferred_element_type=F32).astype(BF16)
        for row, block in following:
            X[row : row + NORM_ROWS, :] = block
        for index, pool in enumerate(pools):
            columns = slice(index * NORM_TILE, (index + 1) * NORM_TILE)
            rounded = pool.astype(BF16)
            PA[at, columns] = rounded
            total = jnp.sum(rounded.astype(F32), axis=0, keepdims=True)
            TA[:, columns] = total if first_row == 0 else TA[:, columns] + total
        for index, query in enumerate(queries):
            at_rows = slice(index * NORM_TILE, (index + 1) * NORM_TILE)
            QA[at_rows, at] = (query * (HEAD_SIZE**-0.5)).astype(BF16).T
        KA[at, :] = both[:, :half_k]
        VA[:, at] = both[:, half_k:].T

    for row in range(0, STEPS[0], NORM_ROWS):
        x_copy(row // BLK).wait()
        X[row : row + NORM_ROWS, :] = normalized(row)
    for b in range(STEPS[0] // BLK, blocks):
        x_copy(b).wait()
    sends[5].start()
    for copy in own:
        copy.wait()
    bounds = (0, *STEPS, rows, rows)
    for step in range(len(bounds) - 2):
        project(*bounds[step : step + 3])

    for copy in sends:
        copy.wait()


def mixer_kernel(
    sp_count,
    X,
    WP,
    WQ,
    WKV,
    WG,
    SK,
    PA,
    QA,
    KA,
    VA,
    TA,
    w_out,
    PART,
    LSR,
    PB,
    PH,
    EARLIER,
    WOP,
    ATT,
    WOA,
    QB,
    KB,
    VB,
    KH,
    VH,
    LS,
    TOT,
    RECV,
    KEEP,
    hsend_sem,
    hrecv_sem,
    tsend_sem,
    trecv_sem,
    lsend_sem,
    lrecv_sem,
    out_sem,
):
    rows, half_k = KB.shape
    half_p, half_q = PA.shape[1], QA.shape[0]
    pw, qw = 2 * half_p, 2 * half_q
    blocks = rows // BLK
    sp, tp = lax.axis_index("sp"), lax.axis_index("tp")
    me = sp * 2 + tp
    count = sp_count * 2
    own_heads = QUERY_HEADS // 2
    first, last = me == 0, me == count - 1

    out_copies = [
        pltpu.make_async_copy(w_out.at[pw : pw + qw], WOA, out_sem.at[0]),
        pltpu.make_async_copy(w_out.at[0:pw], WOP, out_sem.at[1]),
    ]
    for copy in out_copies:
        copy.start()

    barrier = pltpu.get_barrier_semaphore()

    def arrive(device):
        pl.semaphore_signal(barrier, inc=1, device_id=device, device_id_type=MESH)

    arrive({"tp": 1 - tp})
    for distance in range(1, sp_count):
        place = sp + distance
        place = jnp.where(place >= sp_count, place - sp_count, place)
        for core in range(2):
            arrive({"sp": place, "tp": core})

    @pl.when(first)
    def _():
        PH[...] = jnp.zeros_like(PH)
        KH[...] = jnp.zeros_like(KH)
        VH[...] = jnp.zeros_like(VH)

    tile = jnp.dot(X[...], WP[...], preferred_element_type=F32).astype(BF16)
    PB[...] = tile
    TOT[pl.ds(tp, 1), 0] = TA[...]
    TOT[pl.ds(1 - tp, 1), 0] = jnp.sum(tile.astype(F32), axis=0, keepdims=True)
    tile = jnp.dot(X[...], WKV[...], preferred_element_type=F32).astype(BF16)
    KB[...] = tile[:, :half_k]
    VB[...] = tile[:, half_k:].T
    tile = jnp.dot(X[...], WQ[...], preferred_element_type=F32) * (HEAD_SIZE**-0.5)
    QB[...] = tile.astype(BF16).T

    tail = slice(rows - BLK, rows)
    following = lax.rem(sp + tp, sp_count)
    halo_copies = [
        pltpu.make_async_remote_copy(
            src_ref=src,
            dst_ref=dst,
            send_sem=hsend_sem.at[i],
            recv_sem=hrecv_sem.at[i],
            device_id={"sp": following, "tp": 1 - tp},
            device_id_type=MESH,
        )
        for i, (src, dst) in enumerate(
            (
                (KA.at[tail, :], KH.at[1]),
                (KB.at[tail, :], KH.at[0]),
                (VA.at[:, tail], VH.at[1]),
                (VB.at[:, tail], VH.at[0]),
                (PA.at[rows - HALO : rows], PH.at[1]),
                (PB.at[rows - HALO : rows], PH.at[0]),
            )
        )
    ]

    def total_copy(place, core, source):
        return pltpu.make_async_remote_copy(
            src_ref=TOT,
            dst_ref=RECV.at[source],
            send_sem=tsend_sem.at[place * 2 + core],
            recv_sem=trecv_sem.at[source],
            device_id={"sp": place, "tp": core},
            device_id_type=MESH,
        )

    def for_later(act):
        @pl.when(tp == 0)
        def _():
            act(sp, 1)

        @pl.loop(sp + 1, sp_count)
        def _(place):
            act(place, 0)
            act(place, 1)

    def send_out():
        pl.semaphore_wait(barrier, count - 1)

        @pl.when(jnp.logical_not(last))
        def _():
            for copy in halo_copies:
                copy.start()

        for_later(lambda place, core: total_copy(place, core, me).start())

    pairs = 2 * BLK
    older = lax.broadcasted_iota(jnp.int32, (BLK, pairs), 0) > (
        lax.broadcasted_iota(jnp.int32, (BLK, pairs), 1) & (BLK - 1)
    )
    KEEP[0] = jnp.where(older, 1.0, 0.0).astype(BF16)
    KEEP[1] = jnp.where(older, 0.0, 1.0).astype(BF16)
    per_kv = QUERY_HEADS // KEY_VALUE_HEADS

    def query_rows(h, ahead):
        source, row = (QA, h) if h < own_heads else (QB, h - own_heads)
        return source[row * HEAD_SIZE : (row + 1) * HEAD_SIZE, ahead]

    kv_side = KEY_VALUE_HEADS // 2

    def attend(*spec, done=None):
        ready = []
        if done is not None:
            at = pl.ds(pl.multiple_of(done * 2 * BLK, 2 * BLK), 2 * BLK)
            attended = ATT[at, :]
        units = []
        for b, hide in spec:
            start = pl.multiple_of(b * BLK, BLK)
            for h in range(0, QUERY_HEADS, 2):
                units.append((start, hide, h))
        parts = {}

        def ask(index):
            start, hide, h = units[index]
            ahead = pl.ds(start, BLK)
            both = pl.ds(pl.multiple_of(start - BLK, BLK), 2 * BLK)
            side, slot = divmod(h // per_kv, kv_side)
            keys, values = (KA, VA) if side == 0 else (KB, VB)
            at_head = slice(slot * HEAD_SIZE, (slot + 1) * HEAD_SIZE)
            if hide is None:
                key_part, value_part = keys[both, at_head], values[at_head, both]
            else:
                key_part = jnp.concatenate([KH[side, :, at_head], keys[0:BLK, at_head]], axis=0)
                value_part = jnp.concatenate([VH[side, at_head, :], values[at_head, 0:BLK]], axis=1)
            query_part = jnp.concatenate([query_rows(h, ahead), query_rows(h + 1, ahead)], axis=1)
            sink = jnp.concatenate([SK[h : h + 1, :], SK[h + 1 : h + 2, :]], axis=1)
            score = jnp.dot(key_part, query_part, preferred_element_type=F32)
            parts[index] = (ahead, hide, h, score, value_part, sink)

        lead = AHEAD if done is None else AHEAD // 2
        for index in range(min(lead, len(units))):
            ask(index)
        results = []
        for index in range(len(units)):
            ahead, hide, h, score, value_part, sink = parts.pop(index)
            if done is not None and index % 2 == 0:
                n = (index // 2) * GDIM
                ready.append(
                    jnp.dot(attended, WOA[:, n : n + GDIM], preferred_element_type=F32)
                )
            before = score[:BLK]
            if hide is not None:
                before = before + hide
            merged = jnp.where(older, before, score[BLK:])
            row_max = jnp.maximum(jnp.max(merged, axis=0, keepdims=True), sink)
            weights = jnp.exp(merged - row_max)
            weight_sum = jnp.sum(weights, axis=0, keepdims=True) + jnp.exp(sink - row_max)
            rounded = weights.astype(BF16)
            if index + lead < len(units):
                ask(index + lead)
            spread = jnp.concatenate([rounded * KEEP[0], rounded * KEEP[1]], axis=0)
            mixed = jnp.dot(value_part, spread, preferred_element_type=F32)
            mixed = mixed * (1.0 / weight_sum)
            stacked = jnp.concatenate([mixed[:, :BLK], mixed[:, BLK:]], axis=0).astype(BF16)
            results.append((ahead, h, stacked.T, row_max + jnp.log(weight_sum)))
        for n, part in enumerate(ready):
            PART[at, n * GDIM : (n + 1) * GDIM] = part
        for ahead, h, out, logs in results:
            LS[h : h + 1, ahead] = logs[:, :BLK]
            LS[h + 1 : h + 2, ahead] = logs[:, BLK:]
            column = lax.rem(tp * half_q + h * HEAD_SIZE, qw)
            ATT[ahead, pl.ds(pl.multiple_of(column, 128), 2 * HEAD_SIZE)] = out

    def share(first_row, last_row):
        for n in range(0, PART.shape[1], OUT_TILE):
            PART[first_row:last_row, n : n + OUT_TILE] = jnp.dot(
                ATT[first_row:last_row, :], WOA[:, n : n + OUT_TILE], preferred_element_type=F32
            )

    @pl.when(me >= 0)
    def _():
        attend((2, None), (3, None))

    send_out()
    for copy in out_copies:
        copy.wait()

    @pl.loop(2, blocks // 2)
    def _(b):
        attend((2 * b, None), (2 * b + 1, None), done=b - 1)

    @pl.when(jnp.logical_not(first))
    def _():
        for copy in halo_copies:
            copy.wait_recv()

    attend((1, None), (0, jnp.where(first, -jnp.inf, 0.0).astype(F32)), done=blocks // 2 - 1)

    mine = pl.ds(pl.multiple_of(tp * rows, 128), rows)
    log_swap = pltpu.make_async_remote_copy(
        src_ref=LS.at[own_heads : 2 * own_heads, :],
        dst_ref=LSR.at[:, mine],
        send_sem=lsend_sem,
        recv_sem=lrecv_sem,
        device_id={"tp": 1 - tp},
        device_id_type=MESH,
    )
    log_swap.start()
    LSR[:, mine] = LS[0:own_heads, :]

    share(0, 2 * BLK)

    @pl.loop(0, sp)
    def _(place):
        total_copy(place, 0, place * 2).wait_recv()
        total_copy(place, 1, place * 2 + 1).wait_recv()

    @pl.when(tp == 1)
    def _():
        total_copy(sp, 0, sp * 2).wait_recv()

    earlier = jnp.zeros(EARLIER.shape, F32)
    for source in range(count - 1):
        earlier += jnp.where(source < me, RECV[source], 0.0)
    EARLIER[...] = earlier

    log_swap.wait()

    @pl.when(jnp.logical_not(last))
    def _():
        for copy in halo_copies:
            copy.wait_send()

    for_later(lambda place, core: total_copy(place, core, me).wait_send())


def output_kernel(
    PA,
    PB,
    PH,
    before,
    WG,
    WOP,
    PART,
    logs,
    mixed_out,
    logs_out,
    POOL,
    MIXED,
    EARLIER,
    BAND,
    out_sem,
    log_sem,
):
    rows, half_p = PA.shape
    width = MIXED.shape[1]
    blocks = rows // BLK
    tp = lax.axis_index("tp")
    me = lax.axis_index("sp") * 2 + tp
    log_copy = pltpu.make_async_copy(logs, logs_out, log_sem)
    log_copy.start()

    span = HALO + BLK
    back = (
        lax.broadcasted_iota(jnp.int32, (BLK, span), 0)
        + HALO
        - lax.broadcasted_iota(jnp.int32, (BLK, span), 1)
    )
    in_block = lax.broadcasted_iota(jnp.int32, (BLK, span), 1) >= HALO
    prefix_ones = jnp.where((back >= 0) & in_block, 1.0, 0.0).astype(BF16)
    groups = [lax.rem(2 * tp + j, GROUPS) for j in range(GROUPS)]
    reaches = [jnp.left_shift(jnp.int32(2), group) for group in groups]
    for j, reach in enumerate(reaches):
        BAND[j, 0:BLK, :] = jnp.where(
            (back >= 0) & (back < reach), 1.0 / reach.astype(F32), 0.0
        ).astype(BF16)
        BAND[j, BLK : 2 * BLK, :] = prefix_ones

    EARLIER[...] = before[...]
    local_row = lax.broadcasted_iota(jnp.int32, (BLK, 128), 0)
    pair = 2 * BLK

    def pair_rows(index):
        return pl.ds(pl.multiple_of(index * pair, pair), pair)

    def out_copy(index):
        at = pair_rows(index)
        return pltpu.make_async_copy(MIXED.at[at], mixed_out.at[at], out_sem.at[index])

    def step(done, spec):
        units = []
        for b, opening in spec:
            start = pl.multiple_of(b * BLK, BLK)
            for j in range(GROUPS):
                side, at_group = j // 2, slice((j % 2) * GDIM, (j % 2 + 1) * GDIM)
                held = PA if side == 0 else PB
                if opening:
                    source = jnp.concatenate([PH[side, :, at_group], held[0:BLK, at_group]], axis=0)
                else:
                    source = held[pl.ds(pl.multiple_of(start - HALO, HALO), span), at_group]
                units.append((b, opening, j, source))
        sides = [pl.ds(tp if j < 2 else 1 - tp, 1) for j in range(GROUPS)]
        carries = [
            EARLIER[sides[j], 0, (j % 2) * GDIM : (j % 2 + 1) * GDIM] for j in range(GROUPS)
        ]
        sums = [
            jnp.dot(BAND[j], source, preferred_element_type=F32) for b, opening, j, source in units
        ]
        rates = {}
        for b, opening in spec:
            seen = (me * rows + b * BLK + 1 + local_row).astype(F32)
            rates[id(b)] = (seen, 1.0 / seen)
        outs, parts = [], []

        def pool_unit(index):
            b, opening, j, source = units[index]
            seen, per_seen = rates[id(b)]
            window_mean = sums[index][:BLK]
            if opening:
                reach = reaches[j].astype(F32)
                fewer = reach / jnp.minimum(seen, reach)
                window_mean = window_mean * jnp.concatenate([fewer, fewer], axis=1)
            prefix = sums[index][BLK:] + carries[j]
            carries[j] = prefix[BLK - 1 : BLK, :]
            rate = jnp.concatenate([per_seen, per_seen], axis=1)
            pooled = (window_mean - prefix * rate).astype(BF16)
            out = jnp.dot(pooled, WG[j], preferred_element_type=F32).astype(BF16)
            outs.append((pl.ds(pl.multiple_of(b * BLK, BLK), BLK), groups[j], out))

        tiles = range(0, width, GDIM) if done is not None else ()
        for index, n in enumerate(tiles):
            ready = jnp.dot(POOL[pair_rows(done), :], WOP[:, n : n + GDIM], preferred_element_type=F32)
            parts.append((n, (ready + PART[pair_rows(done), n : n + GDIM]).astype(BF16)))
            if index < len(units):
                pool_unit(index)
        for index in range(len(tiles), len(units)):
            pool_unit(index)
        for n, part in parts:
            MIXED[pair_rows(done), n : n + GDIM] = part
        if units:
            for j in range(GROUPS):
                EARLIER[sides[j], 0, (j % 2) * GDIM : (j % 2 + 1) * GDIM] = carries[j]
        for at, group, out in outs:
            POOL[at, pl.ds(pl.multiple_of(group * GDIM, GDIM), GDIM)] = out
        if done is not None:
            out_copy(done).start()

    step(None, ((0, True), (1, False)))

    @pl.loop(1, blocks // 2)
    def _(index):
        step(index - 1, ((2 * index, False), (2 * index + 1, False)))

    step(blocks // 2 - 1, ())
    for index in range(blocks // 2):
        out_copy(index).wait()
    log_copy.wait()


def body(sp_count, tokens, norm_gain, w_query, w_key, w_value, w_pool, w_group, w_out, sinks):
    token_rows = tokens[0]
    both_rows, width = token_rows.shape
    rows = both_rows // 2
    pw, qw, kw = 2 * w_pool.shape[1], 2 * w_query.shape[1], 2 * w_key.shape[1]
    count = sp_count * 2
    blocks = rows // BLK
    hbm = pl.BlockSpec(memory_space=pltpu.HBM)
    vmem = pl.BlockSpec(memory_space=pltpu.VMEM)
    dma = pltpu.SemaphoreType.DMA
    arguments = (
        token_rows,
        norm_gain[None, :],
        w_query,
        w_key,
        w_value,
        w_pool,
        w_group,
        sinks,
    )
    projected = pl.pallas_call(
        project_kernel,
        out_shape=(
            jax.ShapeDtypeStruct((rows, width), BF16),
            jax.ShapeDtypeStruct((width, pw // 2), BF16),
            jax.ShapeDtypeStruct((width, qw // 2), BF16),
            jax.ShapeDtypeStruct((width, kw), BF16),
            jax.ShapeDtypeStruct((GROUPS, GDIM, GDIM), BF16),
            jax.ShapeDtypeStruct((QUERY_HEADS, 128), F32),
            jax.ShapeDtypeStruct((rows, pw // 2), BF16),
            jax.ShapeDtypeStruct((qw // 2, rows), BF16),
            jax.ShapeDtypeStruct((rows, kw // 2), BF16),
            jax.ShapeDtypeStruct((kw // 2, rows), BF16),
            jax.ShapeDtypeStruct((1, pw // 2), F32),
        ),
        in_specs=[hbm] * 8,
        out_specs=(vmem,) * 11,
        scratch_shapes=[
            pltpu.VMEM((1, width), F32),
            pltpu.VMEM((8, width), F32),
            pltpu.SMEM((QUERY_HEADS // 2,), F32),
            pltpu.VMEM((width, pw // 2), BF16),
            pltpu.VMEM((width, qw // 2), BF16),
            pltpu.VMEM((width, kw), BF16),
            dma((blocks,)),
            dma((5,)),
            dma((2,)),
            dma((6,)),
            dma((6,)),
        ],
        compiler_params=pltpu.CompilerParams(
            collective_id=0, has_side_effects=True, vmem_limit_bytes=20 * 2**20
        ),
        name="project",
    )(*(pltpu.with_memory_space_constraint(array, pltpu.HBM) for array in arguments))

    part, logs, other_pool, pool_halo, earlier, pool_weights = pl.pallas_call(
        functools.partial(mixer_kernel, sp_count),
        out_shape=(
            jax.ShapeDtypeStruct((rows, w_out.shape[1]), F32),
            jax.ShapeDtypeStruct((QUERY_HEADS // 2, both_rows), F32),
            jax.ShapeDtypeStruct((rows, pw // 2), BF16),
            jax.ShapeDtypeStruct((2, HALO, pw // 2), BF16),
            jax.ShapeDtypeStruct((2, 1, pw // 2), F32),
            jax.ShapeDtypeStruct((pw, w_out.shape[1]), BF16),
        ),
        in_specs=[vmem] * 11 + [hbm],
        out_specs=(vmem,) * 6,
        scratch_shapes=[
            pltpu.VMEM((rows, qw), BF16),
            pltpu.VMEM((qw, w_out.shape[1]), BF16),
            pltpu.VMEM((qw // 2, rows), BF16),
            pltpu.VMEM((rows, kw // 2), BF16),
            pltpu.VMEM((kw // 2, rows), BF16),
            pltpu.VMEM((2, BLK, kw // 2), BF16),
            pltpu.VMEM((2, kw // 2, BLK), BF16),
            pltpu.VMEM((QUERY_HEADS, rows), F32),
            pltpu.VMEM((2, 1, pw // 2), F32),
            pltpu.VMEM((count, 2, 1, pw // 2), F32),
            pltpu.VMEM((2, BLK, 2 * BLK), BF16),
            dma((6,)),
            dma((6,)),
            dma((count,)),
            dma((count,)),
            dma,
            dma,
            dma((2,)),
        ],
        compiler_params=pltpu.CompilerParams(
            collective_id=1, has_side_effects=True, vmem_limit_bytes=20 * 2**20
        ),
        name="mixers",
    )(*projected, pltpu.with_memory_space_constraint(w_out, pltpu.HBM))

    mixed, log_sums = pl.pallas_call(
        output_kernel,
        out_shape=(
            jax.ShapeDtypeStruct((rows, w_out.shape[1]), BF16),
            jax.ShapeDtypeStruct((QUERY_HEADS // 2, both_rows), F32),
        ),
        in_specs=[vmem] * 8,
        out_specs=(hbm, hbm),
        scratch_shapes=[
            pltpu.VMEM((rows, pw), BF16),
            pltpu.VMEM((rows, w_out.shape[1]), BF16),
            pltpu.VMEM((2, 1, pw // 2), F32),
            pltpu.VMEM((GROUPS, 2 * BLK, HALO + BLK), BF16),
            dma((blocks // 2,)),
            dma,
        ],
        compiler_params=pltpu.CompilerParams(vmem_limit_bytes=24 * 2**20),
        name="output",
    )(
        projected[PA_INDEX],
        other_pool,
        pool_halo,
        earlier,
        projected[WG_INDEX],
        pool_weights,
        part,
        logs,
    )
    return mixed[None], log_sums[None]


def solution(mesh):
    return jax.shard_map(
        functools.partial(body, mesh.shape["sp"]),
        mesh=mesh,
        in_specs=(
            P("fs", "sp", None),
            P(),
            P(None, "tp"),
            P(None, "tp"),
            P(None, "tp"),
            P(None, "tp"),
            P("tp", None, None),
            P(),
            P("tp"),
        ),
        out_specs=(P("fs", ("sp", "tp"), None), P("fs", "tp", "sp")),
        check_vma=False,
    )
```

```python
import functools

import jax
import jax.numpy as jnp
from jax import lax
from jax.experimental import pallas as pl
from jax.experimental.pallas import tpu as pltpu
from jax.sharding import PartitionSpec as P

HEAD_SIZE = 64
GROUPS = 4
GDIM = 256
WINDOW_KEYS = 128
QUERY_HEADS = 16
KEY_VALUE_HEADS = 4
LN_EPS = 1e-05

BLK = 128
HALO = 16
TILE = 256
F32, BF16 = jnp.float32, jnp.bfloat16


MESH = pl.DeviceIdType.MESH
NORM_ROWS = 128
NORM_TILE = 256
OUT_TILE = 512
WG_INDEX, PA_INDEX = 4, 6
STEPS = (640,)
AHEAD = 8


def project_kernel(
    tok,
    gain,
    w_query,
    w_key,
    w_value,
    w_pool,
    w_group,
    sinks,
    X,
    WP,
    WQ,
    WKV,
    WG,
    SK,
    PA,
    QA,
    KA,
    VA,
    TA,
    GAIN,
    GAINS,
    SINK,
    WPO,
    WQO,
    WKVO,
    x_sem,
    w_sem,
    small_sem,
    send_sem,
    recv_sem,
):
    rows, width = X.shape
    blocks = rows // BLK
    half_p, half_q, half_k = PA.shape[1], QA.shape[0], KA.shape[1]
    own_heads = QUERY_HEADS // 2
    tp = lax.axis_index("tp")
    peer = {"tp": 1 - tp}

    barrier = pltpu.get_barrier_semaphore()
    pl.semaphore_signal(barrier, inc=1, device_id=peer, device_id_type=MESH)

    small = [
        pltpu.make_async_copy(gain, GAIN, small_sem.at[0]),
        pltpu.make_async_copy(sinks, SINK, small_sem.at[1]),
    ]
    for copy in small:
        copy.start()

    def x_copy(b):
        return pltpu.make_async_copy(
            tok.at[pl.ds(pl.multiple_of(tp * rows + b * BLK, BLK), BLK), :],
            X.at[b * BLK : (b + 1) * BLK, :],
            x_sem.at[b],
        )

    for b in range(blocks):
        x_copy(b).start()

    pl.semaphore_wait(barrier, 1)
    sends = [
        pltpu.make_async_remote_copy(
            src_ref=src,
            dst_ref=dst,
            send_sem=send_sem.at[i],
            recv_sem=recv_sem.at[i],
            device_id=peer,
            device_id_type=MESH,
        )
        for i, (src, dst) in enumerate(
            (
                (w_pool, WP),
                (w_key, WKV.at[:, 0:half_k]),
                (w_value, WKV.at[:, half_k : 2 * half_k]),
                (w_query, WQ),
                (w_group, WG.at[GROUPS // 2 : GROUPS]),
                (SK.at[0:own_heads], SK.at[own_heads : 2 * own_heads]),
            )
        )
    ]
    for copy in sends[:5]:
        copy.start()

    own = [
        pltpu.make_async_copy(src, dst, w_sem.at[i])
        for i, (src, dst) in enumerate(
            (
                (w_pool, WPO),
                (w_query, WQO),
                (w_key, WKVO.at[:, 0:half_k]),
                (w_value, WKVO.at[:, half_k : 2 * half_k]),
                (w_group, WG.at[0 : GROUPS // 2]),
            )
        )
    ]
    for copy in own:
        copy.start()

    for copy in small:
        copy.wait()
    row_of = lax.broadcasted_iota(jnp.int32, (own_heads, 128), 0)
    sink_block = jnp.zeros((own_heads, 128), F32)
    for h in range(own_heads):
        sink_block = jnp.where(row_of == h, SINK[h], sink_block)
    SK[0:own_heads, :] = sink_block

    GAINS[...] = jnp.broadcast_to(GAIN[...], GAINS.shape)

    def normalized(row):
        values = X[row : row + NORM_ROWS, :].astype(F32)
        mean = jnp.sum(values, axis=-1, keepdims=True) * (1.0 / width)
        centered = values - mean
        variance = jnp.sum(centered * centered, axis=-1, keepdims=True) * (1.0 / width)
        scaled = (centered * lax.rsqrt(variance + LN_EPS)).reshape(-1, 8, width)
        return (scaled * GAINS[...][None]).reshape(NORM_ROWS, width).astype(BF16)

    def project(first_row, last_row, normed_to):
        at = slice(first_row, last_row)
        todo = list(range(last_row, normed_to, NORM_ROWS))
        slots = (half_p + half_q) // NORM_TILE
        following, pools, queries = [], [], []
        rows_in = X[at, :]

        def norm_some(slot):
            for row in todo[len(todo) * slot // slots : len(todo) * (slot + 1) // slots]:
                following.append((row, normalized(row)))

        for n in range(0, half_p, NORM_TILE):
            pools.append(jnp.dot(rows_in, WPO[:, n : n + NORM_TILE], preferred_element_type=F32))
            norm_some(n // NORM_TILE)
        for n in range(0, half_q, NORM_TILE):
            queries.append(jnp.dot(rows_in, WQO[:, n : n + NORM_TILE], preferred_element_type=F32))
            norm_some((half_p + n) // NORM_TILE)
        both = jnp.dot(rows_in, WKVO[...], preferred_element_type=F32).astype(BF16)
        for row, block in following:
            X[row : row + NORM_ROWS, :] = block
        for index, pool in enumerate(pools):
            columns = slice(index * NORM_TILE, (index + 1) * NORM_TILE)
            rounded = pool.astype(BF16)
            PA[at, columns] = rounded
            total = jnp.sum(rounded.astype(F32), axis=0, keepdims=True)
            TA[:, columns] = total if first_row == 0 else TA[:, columns] + total
        for index, query in enumerate(queries):
            at_rows = slice(index * NORM_TILE, (index + 1) * NORM_TILE)
            QA[at_rows, at] = (query * (HEAD_SIZE**-0.5)).astype(BF16).T
        KA[at, :] = both[:, :half_k]
        VA[:, at] = both[:, half_k:].T

    for row in range(0, STEPS[0], NORM_ROWS):
        x_copy(row // BLK).wait()
        X[row : row + NORM_ROWS, :] = normalized(row)
    for b in range(STEPS[0] // BLK, blocks):
        x_copy(b).wait()
    sends[5].start()
    for copy in own:
        copy.wait()
    bounds = (0, *STEPS, rows, rows)
    for step in range(len(bounds) - 2):
        project(*bounds[step : step + 3])

    for copy in sends:
        copy.wait()


def mixer_kernel(
    sp_count,
    X,
    WP,
    WQ,
    WKV,
    WG,
    SK,
    PA,
    QA,
    KA,
    VA,
    TA,
    w_out,
    PART,
    LSR,
    PB,
    PH,
    EARLIER,
    WOP,
    ATT,
    WOA,
    QB,
    KB,
    VB,
    KH,
    VH,
    LS,
    TOT,
    RECV,
    KEEP,
    hsend_sem,
    hrecv_sem,
    tsend_sem,
    trecv_sem,
    lsend_sem,
    lrecv_sem,
    out_sem,
):
    rows, half_k = KB.shape
    half_p, half_q = PA.shape[1], QA.shape[0]
    pw, qw = 2 * half_p, 2 * half_q
    blocks = rows // BLK
    sp, tp = lax.axis_index("sp"), lax.axis_index("tp")
    me = sp * 2 + tp
    count = sp_count * 2
    own_heads = QUERY_HEADS // 2
    first, last = me == 0, me == count - 1

    out_copies = [
        pltpu.make_async_copy(w_out.at[pw : pw + qw], WOA, out_sem.at[0]),
        pltpu.make_async_copy(w_out.at[0:pw], WOP, out_sem.at[1]),
    ]
    for copy in out_copies:
        copy.start()

    barrier = pltpu.get_barrier_semaphore()

    def arrive(device):
        pl.semaphore_signal(barrier, inc=1, device_id=device, device_id_type=MESH)

    arrive({"tp": 1 - tp})
    for distance in range(1, sp_count):
        place = sp + distance
        place = jnp.where(place >= sp_count, place - sp_count, place)
        for core in range(2):
            arrive({"sp": place, "tp": core})

    @pl.when(first)
    def _():
        PH[...] = jnp.zeros_like(PH)
        KH[...] = jnp.zeros_like(KH)
        VH[...] = jnp.zeros_like(VH)

    tile = jnp.dot(X[...], WP[...], preferred_element_type=F32).astype(BF16)
    PB[...] = tile
    TOT[pl.ds(tp, 1), 0] = TA[...]
    TOT[pl.ds(1 - tp, 1), 0] = jnp.sum(tile.astype(F32), axis=0, keepdims=True)
    tile = jnp.dot(X[...], WKV[...], preferred_element_type=F32).astype(BF16)
    KB[...] = tile[:, :half_k]
    VB[...] = tile[:, half_k:].T
    tile = jnp.dot(X[...], WQ[...], preferred_element_type=F32) * (HEAD_SIZE**-0.5)
    QB[...] = tile.astype(BF16).T

    tail = slice(rows - BLK, rows)
    following = lax.rem(sp + tp, sp_count)
    halo_copies = [
        pltpu.make_async_remote_copy(
            src_ref=src,
            dst_ref=dst,
            send_sem=hsend_sem.at[i],
            recv_sem=hrecv_sem.at[i],
            device_id={"sp": following, "tp": 1 - tp},
            device_id_type=MESH,
        )
        for i, (src, dst) in enumerate(
            (
                (KA.at[tail, :], KH.at[1]),
                (KB.at[tail, :], KH.at[0]),
                (VA.at[:, tail], VH.at[1]),
                (VB.at[:, tail], VH.at[0]),
                (PA.at[rows - HALO : rows], PH.at[1]),
                (PB.at[rows - HALO : rows], PH.at[0]),
            )
        )
    ]

    def total_copy(place, core, source):
        return pltpu.make_async_remote_copy(
            src_ref=TOT,
            dst_ref=RECV.at[source],
            send_sem=tsend_sem.at[place * 2 + core],
            recv_sem=trecv_sem.at[source],
            device_id={"sp": place, "tp": core},
            device_id_type=MESH,
        )

    def for_later(act):
        @pl.when(tp == 0)
        def _():
            act(sp, 1)

        @pl.loop(sp + 1, sp_count)
        def _(place):
            act(place, 0)
            act(place, 1)

    def send_out():
        pl.semaphore_wait(barrier, count - 1)

        @pl.when(jnp.logical_not(last))
        def _():
            for copy in halo_copies:
                copy.start()

        for_later(lambda place, core: total_copy(place, core, me).start())

    pairs = 2 * BLK
    older = lax.broadcasted_iota(jnp.int32, (BLK, pairs), 0) > (
        lax.broadcasted_iota(jnp.int32, (BLK, pairs), 1) & (BLK - 1)
    )
    KEEP[0] = jnp.where(older, 1.0, 0.0).astype(BF16)
    KEEP[1] = jnp.where(older, 0.0, 1.0).astype(BF16)
    per_kv = QUERY_HEADS // KEY_VALUE_HEADS

    def query_rows(h, ahead):
        source, row = (QA, h) if h < own_heads else (QB, h - own_heads)
        return source[row * HEAD_SIZE : (row + 1) * HEAD_SIZE, ahead]

    kv_side = KEY_VALUE_HEADS // 2

    def attend(*spec, done=None):
        ready = []
        if done is not None:
            at = pl.ds(pl.multiple_of(done * 2 * BLK, 2 * BLK), 2 * BLK)
            attended = ATT[at, :]
        units = []
        for b, hide in spec:
            start = pl.multiple_of(b * BLK, BLK)
            for h in range(0, QUERY_HEADS, 2):
                units.append((start, hide, h))
        parts = {}

        def ask(index):
            start, hide, h = units[index]
            ahead = pl.ds(start, BLK)
            both = pl.ds(pl.multiple_of(start - BLK, BLK), 2 * BLK)
            side, slot = divmod(h // per_kv, kv_side)
            keys, values = (KA, VA) if side == 0 else (KB, VB)
            at_head = slice(slot * HEAD_SIZE, (slot + 1) * HEAD_SIZE)
            if hide is None:
                key_part, value_part = keys[both, at_head], values[at_head, both]
            else:
                key_part = jnp.concatenate([KH[side, :, at_head], keys[0:BLK, at_head]], axis=0)
                value_part = jnp.concatenate([VH[side, at_head, :], values[at_head, 0:BLK]], axis=1)
            query_part = jnp.concatenate([query_rows(h, ahead), query_rows(h + 1, ahead)], axis=1)
            sink = jnp.concatenate([SK[h : h + 1, :], SK[h + 1 : h + 2, :]], axis=1)
            score = jnp.dot(key_part, query_part, preferred_element_type=F32)
            parts[index] = (ahead, hide, h, score, value_part, sink)

        lead = AHEAD if done is None else AHEAD // 2
        for index in range(min(lead, len(units))):
            ask(index)
        results = []
        for index in range(len(units)):
            ahead, hide, h, score, value_part, sink = parts.pop(index)
            if done is not None and index % 2 == 0:
                n = (index // 2) * GDIM
                ready.append(
                    jnp.dot(attended, WOA[:, n : n + GDIM], preferred_element_type=F32)
                )
            before = score[:BLK]
            if hide is not None:
                before = before + hide
            merged = jnp.where(older, before, score[BLK:])
            row_max = jnp.maximum(jnp.max(merged, axis=0, keepdims=True), sink)
            weights = jnp.exp(merged - row_max)
            weight_sum = jnp.sum(weights, axis=0, keepdims=True) + jnp.exp(sink - row_max)
            rounded = weights.astype(BF16)
            if index + lead < len(units):
                ask(index + lead)
            spread = jnp.concatenate([rounded * KEEP[0], rounded * KEEP[1]], axis=0)
            mixed = jnp.dot(value_part, spread, preferred_element_type=F32)
            mixed = mixed * (1.0 / weight_sum)
            stacked = jnp.concatenate([mixed[:, :BLK], mixed[:, BLK:]], axis=0).astype(BF16)
            results.append((ahead, h, stacked.T, row_max + jnp.log(weight_sum)))
        for n, part in enumerate(ready):
            PART[at, n * GDIM : (n + 1) * GDIM] = part
        for ahead, h, out, logs in results:
            LS[h : h + 1, ahead] = logs[:, :BLK]
            LS[h + 1 : h + 2, ahead] = logs[:, BLK:]
            column = lax.rem(tp * half_q + h * HEAD_SIZE, qw)
            ATT[ahead, pl.ds(pl.multiple_of(column, 128), 2 * HEAD_SIZE)] = out

    def share(first_row, last_row):
        for n in range(0, PART.shape[1], OUT_TILE):
            PART[first_row:last_row, n : n + OUT_TILE] = jnp.dot(
                ATT[first_row:last_row, :], WOA[:, n : n + OUT_TILE], preferred_element_type=F32
            )

    @pl.when(me >= 0)
    def _():
        attend((2, None), (3, None))

    send_out()
    for copy in out_copies:
        copy.wait()

    @pl.loop(2, blocks // 2)
    def _(b):
        attend((2 * b, None), (2 * b + 1, None), done=b - 1)

    @pl.when(jnp.logical_not(first))
    def _():
        for copy in halo_copies:
            copy.wait_recv()

    attend((1, None), (0, jnp.where(first, -jnp.inf, 0.0).astype(F32)), done=blocks // 2 - 1)

    mine = pl.ds(pl.multiple_of(tp * rows, 128), rows)
    log_swap = pltpu.make_async_remote_copy(
        src_ref=LS.at[own_heads : 2 * own_heads, :],
        dst_ref=LSR.at[:, mine],
        send_sem=lsend_sem,
        recv_sem=lrecv_sem,
        device_id={"tp": 1 - tp},
        device_id_type=MESH,
    )
    log_swap.start()
    LSR[:, mine] = LS[0:own_heads, :]

    share(0, 2 * BLK)

    @pl.loop(0, sp)
    def _(place):
        total_copy(place, 0, place * 2).wait_recv()
        total_copy(place, 1, place * 2 + 1).wait_recv()

    @pl.when(tp == 1)
    def _():
        total_copy(sp, 0, sp * 2).wait_recv()

    earlier = jnp.zeros(EARLIER.shape, F32)
    for source in range(count - 1):
        earlier += jnp.where(source < me, RECV[source], 0.0)
    EARLIER[...] = earlier

    log_swap.wait()

    @pl.when(jnp.logical_not(last))
    def _():
        for copy in halo_copies:
            copy.wait_send()

    for_later(lambda place, core: total_copy(place, core, me).wait_send())


def output_kernel(
    PA,
    PB,
    PH,
    before,
    WG,
    WOP,
    PART,
    logs,
    mixed_out,
    logs_out,
    POOL,
    MIXED,
    EARLIER,
    BAND,
    out_sem,
    log_sem,
):
    rows, half_p = PA.shape
    width = MIXED.shape[1]
    blocks = rows // BLK
    tp = lax.axis_index("tp")
    me = lax.axis_index("sp") * 2 + tp
    log_copy = pltpu.make_async_copy(logs, logs_out, log_sem)
    log_copy.start()

    span = HALO + BLK
    back = (
        lax.broadcasted_iota(jnp.int32, (BLK, span), 0)
        + HALO
        - lax.broadcasted_iota(jnp.int32, (BLK, span), 1)
    )
    in_block = lax.broadcasted_iota(jnp.int32, (BLK, span), 1) >= HALO
    prefix_ones = jnp.where((back >= 0) & in_block, 1.0, 0.0).astype(BF16)
    groups = [lax.rem(2 * tp + j, GROUPS) for j in range(GROUPS)]
    reaches = [jnp.left_shift(jnp.int32(2), group) for group in groups]
    for j, reach in enumerate(reaches):
        BAND[j, 0:BLK, :] = jnp.where(
            (back >= 0) & (back < reach), 1.0 / reach.astype(F32), 0.0
        ).astype(BF16)
        BAND[j, BLK : 2 * BLK, :] = prefix_ones

    EARLIER[...] = before[...]
    local_row = lax.broadcasted_iota(jnp.int32, (BLK, 128), 0)
    pair = 2 * BLK

    def pair_rows(index):
        return pl.ds(pl.multiple_of(index * pair, pair), pair)

    def out_copy(index):
        at = pair_rows(index)
        return pltpu.make_async_copy(MIXED.at[at], mixed_out.at[at], out_sem.at[index])

    def step(done, spec):
        units = []
        for b, opening in spec:
            start = pl.multiple_of(b * BLK, BLK)
            for j in range(GROUPS):
                side, at_group = j // 2, slice((j % 2) * GDIM, (j % 2 + 1) * GDIM)
                held = PA if side == 0 else PB
                if opening:
                    source = jnp.concatenate([PH[side, :, at_group], held[0:BLK, at_group]], axis=0)
                else:
                    source = held[pl.ds(pl.multiple_of(start - HALO, HALO), span), at_group]
                units.append((b, opening, j, source))
        sides = [pl.ds(tp if j < 2 else 1 - tp, 1) for j in range(GROUPS)]
        carries = [
            EARLIER[sides[j], 0, (j % 2) * GDIM : (j % 2 + 1) * GDIM] for j in range(GROUPS)
        ]
        sums = [
            jnp.dot(BAND[j], source, preferred_element_type=F32) for b, opening, j, source in units
        ]
        rates = {}
        for b, opening in spec:
            seen = (me * rows + b * BLK + 1 + local_row).astype(F32)
            rates[id(b)] = (seen, 1.0 / seen)
        outs, parts = [], []

        def pool_unit(index):
            b, opening, j, source = units[index]
            seen, per_seen = rates[id(b)]
            window_mean = sums[index][:BLK]
            if opening:
                reach = reaches[j].astype(F32)
                fewer = reach / jnp.minimum(seen, reach)
                window_mean = window_mean * jnp.concatenate([fewer, fewer], axis=1)
            prefix = sums[index][BLK:] + carries[j]
            carries[j] = prefix[BLK - 1 : BLK, :]
            rate = jnp.concatenate([per_seen, per_seen], axis=1)
            pooled = (window_mean - prefix * rate).astype(BF16)
            out = jnp.dot(pooled, WG[j], preferred_element_type=F32).astype(BF16)
            outs.append((pl.ds(pl.multiple_of(b * BLK, BLK), BLK), groups[j], out))

        tiles = range(0, width, GDIM) if done is not None else ()
        for index, n in enumerate(tiles):
            ready = jnp.dot(POOL[pair_rows(done), :], WOP[:, n : n + GDIM], preferred_element_type=F32)
            parts.append((n, (ready + PART[pair_rows(done), n : n + GDIM]).astype(BF16)))
            if index < len(units):
                pool_unit(index)
        for index in range(len(tiles), len(units)):
            pool_unit(index)
        for n, part in parts:
            MIXED[pair_rows(done), n : n + GDIM] = part
        if units:
            for j in range(GROUPS):
                EARLIER[sides[j], 0, (j % 2) * GDIM : (j % 2 + 1) * GDIM] = carries[j]
        for at, group, out in outs:
            POOL[at, pl.ds(pl.multiple_of(group * GDIM, GDIM), GDIM)] = out
        if done is not None:
            out_copy(done).start()

    step(None, ((0, True), (1, False)))

    @pl.loop(1, blocks // 2)
    def _(index):
        step(index - 1, ((2 * index, False), (2 * index + 1, False)))

    final = slice(rows - pair, rows)
    cut = width * 3 // 4
    last_copies = []
    for part, columns in enumerate((slice(0, cut), slice(cut, width))):
        ready = jnp.dot(POOL[final, :], WOP[:, columns], preferred_element_type=F32)
        MIXED[final, columns] = (ready + PART[final, columns]).astype(BF16)
        last_copies.append(
            pltpu.make_async_copy(
                MIXED.at[final, columns],
                mixed_out.at[final, columns],
                out_sem.at[blocks // 2 - 1 + part],
            )
        )
        last_copies[part].start()
    for index in range(blocks // 2 - 1):
        out_copy(index).wait()
    for copy in last_copies:
        copy.wait()
    log_copy.wait()


def body(sp_count, tokens, norm_gain, w_query, w_key, w_value, w_pool, w_group, w_out, sinks):
    token_rows = tokens[0]
    both_rows, width = token_rows.shape
    rows = both_rows // 2
    pw, qw, kw = 2 * w_pool.shape[1], 2 * w_query.shape[1], 2 * w_key.shape[1]
    count = sp_count * 2
    blocks = rows // BLK
    hbm = pl.BlockSpec(memory_space=pltpu.HBM)
    vmem = pl.BlockSpec(memory_space=pltpu.VMEM)
    dma = pltpu.SemaphoreType.DMA
    arguments = (
        token_rows,
        norm_gain[None, :],
        w_query,
        w_key,
        w_value,
        w_pool,
        w_group,
        sinks,
    )
    projected = pl.pallas_call(
        project_kernel,
        out_shape=(
            jax.ShapeDtypeStruct((rows, width), BF16),
            jax.ShapeDtypeStruct((width, pw // 2), BF16),
            jax.ShapeDtypeStruct((width, qw // 2), BF16),
            jax.ShapeDtypeStruct((width, kw), BF16),
            jax.ShapeDtypeStruct((GROUPS, GDIM, GDIM), BF16),
            jax.ShapeDtypeStruct((QUERY_HEADS, 128), F32),
            jax.ShapeDtypeStruct((rows, pw // 2), BF16),
            jax.ShapeDtypeStruct((qw // 2, rows), BF16),
            jax.ShapeDtypeStruct((rows, kw // 2), BF16),
            jax.ShapeDtypeStruct((kw // 2, rows), BF16),
            jax.ShapeDtypeStruct((1, pw // 2), F32),
        ),
        in_specs=[hbm] * 8,
        out_specs=(vmem,) * 11,
        scratch_shapes=[
            pltpu.VMEM((1, width), F32),
            pltpu.VMEM((8, width), F32),
            pltpu.SMEM((QUERY_HEADS // 2,), F32),
            pltpu.VMEM((width, pw // 2), BF16),
            pltpu.VMEM((width, qw // 2), BF16),
            pltpu.VMEM((width, kw), BF16),
            dma((blocks,)),
            dma((5,)),
            dma((2,)),
            dma((6,)),
            dma((6,)),
        ],
        compiler_params=pltpu.CompilerParams(
            collective_id=0, has_side_effects=True, vmem_limit_bytes=20 * 2**20
        ),
        name="project",
    )(*(pltpu.with_memory_space_constraint(array, pltpu.HBM) for array in arguments))

    part, logs, other_pool, pool_halo, earlier, pool_weights = pl.pallas_call(
        functools.partial(mixer_kernel, sp_count),
        out_shape=(
            jax.ShapeDtypeStruct((rows, w_out.shape[1]), F32),
            jax.ShapeDtypeStruct((QUERY_HEADS // 2, both_rows), F32),
            jax.ShapeDtypeStruct((rows, pw // 2), BF16),
            jax.ShapeDtypeStruct((2, HALO, pw // 2), BF16),
            jax.ShapeDtypeStruct((2, 1, pw // 2), F32),
            jax.ShapeDtypeStruct((pw, w_out.shape[1]), BF16),
        ),
        in_specs=[vmem] * 11 + [hbm],
        out_specs=(vmem,) * 6,
        scratch_shapes=[
            pltpu.VMEM((rows, qw), BF16),
            pltpu.VMEM((qw, w_out.shape[1]), BF16),
            pltpu.VMEM((qw // 2, rows), BF16),
            pltpu.VMEM((rows, kw // 2), BF16),
            pltpu.VMEM((kw // 2, rows), BF16),
            pltpu.VMEM((2, BLK, kw // 2), BF16),
            pltpu.VMEM((2, kw // 2, BLK), BF16),
            pltpu.VMEM((QUERY_HEADS, rows), F32),
            pltpu.VMEM((2, 1, pw // 2), F32),
            pltpu.VMEM((count, 2, 1, pw // 2), F32),
            pltpu.VMEM((2, BLK, 2 * BLK), BF16),
            dma((6,)),
            dma((6,)),
            dma((count,)),
            dma((count,)),
            dma,
            dma,
            dma((2,)),
        ],
        compiler_params=pltpu.CompilerParams(
            collective_id=1, has_side_effects=True, vmem_limit_bytes=20 * 2**20
        ),
        name="mixers",
    )(*projected, pltpu.with_memory_space_constraint(w_out, pltpu.HBM))

    mixed, log_sums = pl.pallas_call(
        output_kernel,
        out_shape=(
            jax.ShapeDtypeStruct((rows, w_out.shape[1]), BF16),
            jax.ShapeDtypeStruct((QUERY_HEADS // 2, both_rows), F32),
        ),
        in_specs=[vmem] * 8,
        out_specs=(hbm, hbm),
        scratch_shapes=[
            pltpu.VMEM((rows, pw), BF16),
            pltpu.VMEM((rows, w_out.shape[1]), BF16),
            pltpu.VMEM((2, 1, pw // 2), F32),
            pltpu.VMEM((GROUPS, 2 * BLK, HALO + BLK), BF16),
            dma((blocks // 2 + 1,)),
            dma,
        ],
        compiler_params=pltpu.CompilerParams(vmem_limit_bytes=24 * 2**20),
        name="output",
    )(
        projected[PA_INDEX],
        other_pool,
        pool_halo,
        earlier,
        projected[WG_INDEX],
        pool_weights,
        part,
        logs,
    )
    return mixed[None], log_sums[None]


def solution(mesh):
    return jax.shard_map(
        functools.partial(body, mesh.shape["sp"]),
        mesh=mesh,
        in_specs=(
            P("fs", "sp", None),
            P(),
            P(None, "tp"),
            P(None, "tp"),
            P(None, "tp"),
            P(None, "tp"),
            P("tp", None, None),
            P(),
            P("tp"),
        ),
        out_specs=(P("fs", ("sp", "tp"), None), P("fs", "tp", "sp")),
        check_vma=False,
    )
```
